32 devices in a mesh: kv: 16 (over z, y, core), tp: 2 (over x).
Axes of the slice: x: 2, y: 2, z: 4, core: 2. Of those that a mesh axis runs over, the one named last changes fastest.
Arguments:
- queries: bfloat16 [4096, 4, 128], P('kv', 'tp'), may hold values from -6 to 6
- keys: bfloat16 [4096, 4, 128], P('kv', 'tp'), may hold values from -6 to 6
- values: bfloat16 [4096, 4, 128], P('kv', 'tp'), may hold values from -6 to 6
- attended: bfloat16 [4096, 4, 128], P('kv', 'tp'), may hold values from -6 to 6
- out_grad: bfloat16 [4096, 4, 128], P('kv', 'tp'), may hold values from -6 to 6
- log_sum: float32 [4096, 4], P('kv', 'tp'), may hold values from 2.5 to 4.5
- picked: int32 [32, 16], P('kv'), may hold values from -1 to 127, as said below
- layer_input: bfloat16 [4096, 4096], P('kv'), may hold values from -0.03125 to 0.03125
Outputs:
- query_grad: float32 [4096, 4, 128], P('kv', 'tp')
- key_grad: float32 [4096, 4, 128], P('kv', 'tp')
- value_grad: float32 [4096, 4, 128], P('kv', 'tp')
- weight_grad: float32 [4096, 512], P('kv', 'tp')
The draws below stay inside these ranges and needn't reach their ends.
Inputs may be any that keep to these rules, and one draw needn't show every extreme that they name: Row r lists distinct key block numbers picked by query block r, followed by -1 to the end of the row; at least one entry is not -1, and at most 16 are. No picked block starts after the last position of its query block. With the span of a position being the position divided by 256 (rounded down), the span of every picked block is the query block's span or that span less 1, 2, 4, 8 and so on. The query blocks of one span pick at most 4 distinct blocks from any other single span.
All inputs are finite; a program needn't handle non-finite values.
Results may differ from the reference program's by a relative error of at most 0.004.
Values may be sent and summed in bfloat16 or wider, within the bound.
A program may use at most 64 MiB of HBM per device.

```python
import jax
import jax.numpy as jnp
from jax import lax

D = 4096
HEADS = 4
DH = 128
TOK_DEV = 256
QB = 128
KB = 32
MAXSEL = 16
PER_SPAN = 4
TOKENS = 4096
QBLOCKS = 32


def draw_picked(key, part):
    span_count = TOKENS // TOK_DEV
    span_blocks = TOK_DEV // KB
    query_count = TOK_DEV // QB
    levels = span_count.bit_length() - 1
    groups = levels + 1
    slot_total = groups * span_blocks
    allow_key = jax.random.fold_in(key, 11)
    score_key = jax.random.fold_in(key, 12)
    count_key_a = jax.random.fold_in(key, 13)
    count_key_b = jax.random.fold_in(key, 14)
    block_axis = jnp.arange(span_blocks, dtype=jnp.int32)
    allow_scores = jax.random.randint(allow_key, (span_count, groups, span_blocks), 0, 1 << 20, dtype=jnp.int32) * span_blocks + block_axis
    allow_rank = jnp.argsort(jnp.argsort(allow_scores, axis=-1), axis=-1)
    allowed = allow_rank < PER_SPAN
    span_index = jnp.arange(span_count, dtype=jnp.int32)[:, None, None, None]
    query_index = jnp.arange(query_count, dtype=jnp.int32)[None, :, None, None]
    group_index = jnp.arange(groups, dtype=jnp.int32)[None, None, :, None]
    block_index = block_axis[None, None, None, :]
    back_spans = jnp.where(group_index == 0, 0, jnp.left_shift(jnp.ones_like(group_index), jnp.maximum(group_index - 1, 0)))
    owner_span = span_index - back_spans
    own_usable = (group_index == 0) & (block_index * KB <= query_index * QB + QB - 1)
    far_usable = (group_index > 0) & (owner_span >= 0) & allowed[:, None, :, :]
    usable = own_usable | far_usable
    slot_index = group_index * span_blocks + block_index
    draw_scores = jax.random.randint(score_key, (span_count, query_count, groups, span_blocks), 0, 1 << 16, dtype=jnp.int32)
    unique = draw_scores * slot_total + slot_index
    masked = jnp.where(usable, unique, -1)
    group_best = jnp.max(masked, axis=-1, keepdims=True)
    last_query = query_index == query_count - 1
    forced = usable & (masked == group_best) | usable & last_query & (group_index == 1)
    ranked = jnp.where(usable, unique + jnp.where(forced, 1 << 28, 0), -1)
    half_most = MAXSEL // 2
    extra_picks = jax.random.randint(count_key_a, (span_count, query_count), 0, half_most + 1, dtype=jnp.int32) * jax.random.randint(count_key_b, (span_count, query_count), 0, half_most + 1, dtype=jnp.int32) // half_most
    usable_count = jnp.sum(usable.astype(jnp.int32), axis=(2, 3))
    forced_count = jnp.sum(forced.astype(jnp.int32), axis=(2, 3))
    last_row = (jnp.arange(query_count, dtype=jnp.int32) == query_count - 1)[None, :]
    wanted = jnp.where(last_row, MAXSEL, jnp.maximum(half_most + extra_picks, forced_count))
    pick_count = jnp.minimum(wanted, usable_count)
    flat_ranked = ranked.reshape(span_count, query_count, slot_total)
    top_values, top_slots = lax.top_k(flat_ranked, MAXSEL)
    chosen_group = top_slots // span_blocks
    chosen_block = top_slots % span_blocks
    chosen_back = jnp.where(chosen_group == 0, 0, jnp.left_shift(jnp.ones_like(chosen_group), jnp.maximum(chosen_group - 1, 0)))
    chosen_span = jnp.arange(span_count, dtype=jnp.int32)[:, None, None] - chosen_back
    chosen_ids = chosen_span * span_blocks + chosen_block
    position = jnp.arange(MAXSEL, dtype=jnp.int32)[None, None, :]
    chosen_ids = jnp.where(position < pick_count[:, :, None], chosen_ids, -1)
    return chosen_ids.reshape(span_count * query_count, MAXSEL).astype(jnp.int32)


def raised(array, own_key, source, target, shards_of, factor):
    def block_of(axis_at):
        return (jnp.arange(array.shape[axis_at]) // (array.shape[axis_at] // shards_of)).reshape((-1,) + (1,) * (array.ndim - 1 - axis_at))

    one_side = jax.random.permutation(own_key, shards_of)[block_of(target)]
    other_side = (block_of(target) + shards_of // 2) % shards_of
    return jnp.where((block_of(source) == one_side) | (block_of(source) == other_side), factor * array, array)


def level_of(stream_key, extent, split, smallest, high):
    gain, own = 1.0, jax.random.fold_in(stream_key, 6)
    for axis_at, blocks in split:
        draws = jnp.exp(jax.random.uniform(jax.random.fold_in(own, axis_at), (blocks,), jnp.float32, smallest / len(split), high / len(split)))
        gain = gain * jnp.repeat(draws, extent[axis_at] // blocks).reshape([-1 if axis == axis_at else 1 for axis in range(len(extent))])
    return gain


def gaussian(rng, dims, scale, bound, split=(), kind=jnp.bfloat16):
    entries = scale * jax.random.normal(rng, dims, jnp.float32)
    if split:
        entries = entries * level_of(rng, dims, split, -0.22, 0.18)
    return jnp.clip(entries, -bound, bound).astype(kind)


def heavy_noise(key, extent, spread, bound, cuts, heavy, kind=jnp.bfloat16):
    entries = spread * jax.random.normal(key, extent, jnp.float32)
    if cuts:
        entries = entries * level_of(key, extent, cuts, -0.22, 0.18)
    return jnp.clip(raised(entries, jax.random.fold_in(key, 3), *heavy), -bound, bound).astype(kind)


def setup_inputs(seed: int = 0) -> dict:
    arg_keys = jax.random.split(jax.random.key(seed), 9)
    queries = gaussian(arg_keys[0], (TOKENS, HEADS, DH), 1.0, 6.0, ((0, 16), (1, 2)))
    keys = gaussian(arg_keys[1], (TOKENS, HEADS, DH), 1.0, 6.0, ((0, 16), (1, 2)))
    values = gaussian(arg_keys[2], (TOKENS, HEADS, DH), 1.0, 6.0, ((0, 16), (1, 2)))
    attended = gaussian(arg_keys[3], (TOKENS, HEADS, DH), 1.0, 6.0, ((0, 16), (1, 2)))
    out_grad = gaussian(arg_keys[4], (TOKENS, HEADS, DH), 1.0, 6.0, ((0, 16), (1, 2)))
    log_sum = jnp.clip(2.5 + 2.0 * jax.random.uniform(arg_keys[5], (TOKENS, HEADS), jnp.float32) ** level_of(arg_keys[5], (TOKENS, HEADS), ((0, 16), (1, 2)), -0.2, 0.2), 2.5, 4.5)
    picked = draw_picked(jax.random.fold_in(arg_keys[8], 71), 0)
    layer_input = heavy_noise(arg_keys[7], (TOKENS, D), 0.004, 0.03125, ((0, 16),), (0, 1, 16, 2.0))
    return dict(queries=queries, keys=keys, values=values, attended=attended, out_grad=out_grad, log_sum=log_sum, picked=picked, layer_input=layer_input)


def reference(queries, keys, values, attended, out_grad, log_sum, picked, layer_input):
    score_scale = DH ** -0.5
    row_dots = jnp.sum(out_grad.astype(jnp.float32) * attended.astype(jnp.float32), axis=-1)
    key_offsets = jnp.arange(KB, dtype=jnp.int32)
    query_offsets = jnp.arange(QB, dtype=jnp.int32)

    def one_block(carry, block_index):
        key_sums, value_sums = carry
        listed = picked[block_index]
        listed_live = listed >= 0
        gather_rows = (jnp.where(listed_live, listed, 0)[:, None] * KB + key_offsets[None, :]).reshape(-1).astype(jnp.int32)
        key_live = jnp.repeat(listed_live, KB)
        first_query = (block_index * QB).astype(jnp.int32)
        query_pos = first_query + query_offsets
        pair_live = key_live[None, :] & (gather_rows[None, :] <= query_pos[:, None])
        query_rows = lax.dynamic_slice_in_dim(queries, first_query, QB, 0).astype(jnp.float32)
        grad_rows = lax.dynamic_slice_in_dim(out_grad, first_query, QB, 0).astype(jnp.float32)
        stored = lax.dynamic_slice_in_dim(log_sum, first_query, QB, 0)
        block_dots = lax.dynamic_slice_in_dim(row_dots, first_query, QB, 0)
        key_rows = keys[gather_rows].astype(jnp.float32)
        value_rows = values[gather_rows].astype(jnp.float32)
        scores = jnp.einsum("qhd,khd->hqk", query_rows, key_rows) * score_scale
        weights = jnp.where(pair_live[None], jnp.exp(scores - stored.T[:, :, None]), 0.0)
        slopes = jnp.einsum("qhd,khd->hqk", grad_rows, value_rows)
        score_grad = weights * (slopes - block_dots.T[:, :, None])
        weight_pairs = lax.optimization_barrier(weights.astype(jnp.bfloat16)).astype(jnp.float32)
        grad_pairs = lax.optimization_barrier(score_grad.astype(jnp.bfloat16)).astype(jnp.float32)
        query_grad = jnp.einsum("hqk,khd->qhd", grad_pairs, key_rows) * score_scale
        key_terms = jnp.einsum("hqk,qhd->khd", grad_pairs, query_rows) * score_scale
        value_terms = jnp.einsum("hqk,qhd->khd", weight_pairs, grad_rows)
        key_sums = key_sums.at[gather_rows].add(key_terms)
        value_sums = value_sums.at[gather_rows].add(value_terms)
        return (key_sums, value_sums), query_grad

    empty = jnp.zeros(keys.shape, jnp.float32)
    (key_grad, value_grad), query_grad = lax.scan(one_block, (empty, empty), jnp.arange(QBLOCKS, dtype=jnp.int32))
    query_grad = query_grad.reshape(TOKENS, HEADS, DH)
    value_round = value_grad.astype(jnp.bfloat16).reshape(TOKENS, HEADS * DH)
    weight_grad = lax.dot_general(layer_input, value_round, (((0,), (0,)), ((), ())), preferred_element_type=jnp.float32)
    return query_grad, key_grad, value_grad, weight_grad
```

```python
import functools

import jax
import jax.numpy as jnp
from jax import lax
from jax.experimental import pallas as pl
from jax.experimental.pallas import tpu as pltpu
from jax.sharding import PartitionSpec as P

QB = 128
KB = 32
PER_SPAN = 4
COMPACT = PER_SPAN * KB
CHUNKS = 8
F32 = jnp.float32
BF16 = jnp.bfloat16


def xor(value, bits):
    out = value
    for i in range(bits.bit_length()):
        if bits >> i & 1:
            out = out + (1 << i) - (2 << i) * lax.rem(value // (1 << i), 2)
    return out


def dot_nt(a, b):
    return lax.dot_general(a, b, (((1,), (1,)), ((), ())), preferred_element_type=F32)


def dot_tn(a, b):
    return lax.dot_general(a, b, (((0,), (0,)), ((), ())), preferred_element_type=F32)


def dot_nn(a, b):
    return lax.dot_general(a, b, (((1,), (0,)), ((), ())), preferred_element_type=F32)


def body(
    n, levels, heads, dh,
    picked_hbm, q_hbm, k_hbm, v_hbm, att_hbm, og_hbm, log_hbm, x_hbm,
    dq_out, dk_out, dv_out, wg_out,
    picked, log_sum, dq, dk, dv, raw, q, k, v, att, og, x, xt, slot, slot_in, pick, ksend, kin, vsend, vin, dvsend, dvin, dksend, dkin,
    wts, part, got1, send2, got2, send3, got3,
    x_sem, picked_sem, log_sem, raw_sem, slot_ss, slot_rs, k_ss, k_rs, v_ss, v_rs, dv_ss, dv_rs, dk_ss, dk_rs,
    s1_ss, s1_rs, s2_ss, s2_rs, s3_ss, s3_rs,
):
    me = lax.axis_index("kv")
    tok, cols = q.shape
    query_count = tok // QB
    span_blocks = tok // KB
    rows = slot.shape[0]
    scale = dh ** (-0.5)
    quarter = n // 4
    rb = wg_out.shape[0]
    order = list(reversed(range(levels)))

    def to(offset):
        return {"kv": lax.rem(me + offset + n, n)}

    def flipped(bits):
        low = lax.rem(me, 4)
        high = me // 4
        if bits == 1:
            return {"kv": me + 1 - 2 * lax.rem(me, 2)}
        if bits == 2:
            return {"kv": me + 2 - 4 * (low // 2)}
        return {"kv": xor(high, bits // 4) * 4 + low}

    def remote(src, dst, ss, rs, device):
        return pltpu.make_async_remote_copy(
            src_ref=src, dst_ref=dst, send_sem=ss, recv_sem=rs,
            device_id=device, device_id_type=pl.DeviceIdType.MESH,
        )

    load_picked = pltpu.make_async_copy(picked_hbm, picked, picked_sem)
    load_picked.start()
    barrier = pltpu.get_barrier_semaphore()
    greeted = [to(1 << l) for l in range(levels)] + [to(-(1 << l)) for l in range(levels)]
    greeted += [flipped(1), flipped(2)] + [flipped(4 * b) for b in range(1, quarter)]
    for device in greeted:
        pl.semaphore_signal(
            barrier, inc=1, device_id=device, device_id_type=pl.DeviceIdType.MESH
        )

    loads = {}
    for i, (src, dst) in enumerate(
        ((k_hbm, k), (v_hbm, v), (q_hbm, q), (og_hbm, og), (att_hbm, att))
    ):
        loads[i] = (pltpu.make_async_copy(src, raw.at[i], raw_sem.at[i]), dst)
        loads[i][0].start()

    def settle(i):
        copy, dst = loads[i]
        copy.wait()
        for h in range(heads):
            dst[:, h * dh : (h + 1) * dh] = raw[i, :, h, :]

    load_x = pltpu.make_async_copy(x_hbm, x, x_sem)
    load_x.start()
    load_log = pltpu.make_async_copy(log_hbm, log_sum, log_sem)
    load_log.start()
    row = lax.broadcasted_iota(jnp.int32, (rows, tok), 0)
    lane = lax.broadcasted_iota(jnp.int32, (rows, tok), 1)
    back = jnp.zeros((rows, tok), jnp.int32)
    for l in range(levels):
        back = jnp.where(row == l + 1, 1 << l, back)
    ids = jnp.where(row <= levels, (me - back) * span_blocks + lane // KB, -2)
    load_picked.wait()
    live = []
    for b in range(query_count):
        hit = jnp.zeros((rows, tok), jnp.int32)
        for s in range(picked.shape[1]):
            p = picked[b, s]
            hit = jnp.where(ids == jnp.where(p < 0, -(1 << 30), p), 1, hit)
        live.append(hit.astype(F32))
    need = functools.reduce(jnp.maximum, live)
    below = lax.broadcasted_iota(jnp.int32, (tok, tok), 0)
    above = lax.broadcasted_iota(jnp.int32, (tok, tok), 1)
    steps = jnp.where((below % KB == 0) & (below // KB < above // KB), 1.0, 0.0).astype(BF16)
    rank = dot_nn(need.astype(BF16), steps)
    slot[...] = jnp.where(need > 0, rank * KB + (lane % KB).astype(F32), -1.0)

    pl.semaphore_wait(barrier, len(greeted))

    def sends_up(l):
        return me + (1 << l) < n

    def sends_down(l):
        return me >= 1 << l

    slot_copies = {}
    for l in order:
        slot_copies[l] = remote(
            slot, slot_in.at[l], slot_ss.at[l], slot_rs.at[l], to(-(1 << l))
        )
        pl.when(sends_down(l))(slot_copies[l].start)

    settle(0)
    settle(1)

    def one_hot(row_values):
        sub = lax.broadcasted_iota(jnp.int32, (COMPACT, tok), 0).astype(F32)
        return jnp.where(sub == row_values, 1.0, 0.0).astype(BF16)

    head = [slice(h * dh, (h + 1) * dh) for h in range(heads)]
    k_copies, v_copies, dv_copies, dk_copies = {}, {}, {}, {}
    for l in order:
        k_copies[l] = remote(ksend.at[l], kin.at[l], k_ss.at[l], k_rs.at[l], to(1 << l))
        v_copies[l] = remote(vsend.at[l], vin.at[l], v_ss.at[l], v_rs.at[l], to(1 << l))
        dv_copies[l] = remote(
            dvsend.at[l], dvin.at[l], dv_ss.at[l], dv_rs.at[l], to(-(1 << l))
        )
        dk_copies[l] = remote(
            dksend.at[l], dkin.at[l], dk_ss.at[l], dk_rs.at[l], to(-(1 << l))
        )
    for l in order:

        @pl.when(sends_up(l))
        def _(l=l):
            slot_copies[l].wait_recv()
            chosen = one_hot(slot_in[l, l + 1 : l + 2, :])
            pick[l] = chosen
            ksend[l] = dot_nn(chosen, k[...]).astype(BF16)
            k_copies[l].start()

    for l in order:

        @pl.when(sends_up(l))
        def _(l=l):
            vsend[l] = dot_nn(pick[l], v[...]).astype(BF16)
            v_copies[l].start()

    for i in range(2, 5):
        settle(i)
    dots = []
    for c in head:
        column = jnp.sum(og[:, c].astype(F32) * att[:, c].astype(F32), axis=1, keepdims=True)
        dots.append(jnp.transpose(jnp.broadcast_to(column, (tok, 128)))[0:1, :])
    load_log.wait()
    stored = [log_sum[h : h + 1, :] for h in range(heads)]

    def key_mask(chosen, r):
        pieces = []
        for m in live:
            column = dot_nt(chosen, m.astype(BF16))[:, r : r + 1]
            pieces.append(jnp.broadcast_to(column, (column.shape[0], QB)))
        return jnp.concatenate(pieces, axis=1) > 0

    own_mask = key_mask(jnp.where(below == above, 1.0, 0.0).astype(BF16), 0) & (below <= above)
    for h, c in enumerate(head):
        w = jnp.where(own_mask, jnp.exp(dot_nt(k[:, c], q[:, c]) * scale - stored[h]), 0.0)
        dv[:, c] = dot_nn(w.astype(BF16), og[:, c])
        g = (w * (dot_nt(v[:, c], og[:, c]) - dots[h])).astype(BF16)
        dk[:, c] = dot_nn(g, q[:, c])
        dq[:, c] = dot_tn(g, k[:, c])

    masks = {
        l: key_mask(one_hot(slot[l + 1 : l + 2, :]), l + 1) for l in order
    }
    load_x.wait()
    width = x.shape[1] // CHUNKS
    for i in range(CHUNKS):
        xt[i * width : (i + 1) * width, :] = jnp.transpose(x[:, i * width : (i + 1) * width])
    for l in range(levels):

        @pl.when(sends_down(l))
        def _(l=l):
            k_copies[l].wait_recv()
            for h, c in enumerate(head):
                w = jnp.where(
                    masks[l], jnp.exp(dot_nt(kin[l, :, c], q[:, c]) * scale - stored[h]), 0.0
                )
                wts[l, h] = w
                dvsend[l, :, c] = dot_nn(w.astype(BF16), og[:, c]).astype(BF16)
            dv_copies[l].start()

    for l in range(levels):

        @pl.when(sends_down(l))
        def _(l=l):
            v_copies[l].wait_recv()
            for h, c in enumerate(head):
                g = (wts[l, h] * (dot_nt(vin[l, :, c], og[:, c]) - dots[h])).astype(BF16)
                dksend[l, :, c] = (dot_nn(g, q[:, c]) * scale).astype(BF16)
                dq[:, c] += dot_tn(g, kin[l, :, c])
            dk_copies[l].start()

    def emit(src, dst, factor):
        for h, c in enumerate(head):
            dst[pl.ds(h, tok, stride=heads), :] = src[:, c] * factor


    for l in range(levels):

        @pl.when(sends_up(l))
        def _(l=l):
            dv_copies[l].wait_recv()
            dv[...] += dot_tn(pick[l], dvin[l])

    rounded = dv[...].astype(BF16)
    core = lax.rem(me, 2)
    up = lax.rem(me, 4) // 2
    high = me // 4
    far = list(reversed(range(quarter)))
    chunk = 2 * rb
    s1, s2, s3 = [], [], []

    def share(t, at):
        first = pl.multiple_of(at * chunk, chunk)
        w = dot_nn(xt[pl.ds(first, chunk), :], rounded)
        part[t] = w.reshape(2, rb, cols)
        copy = remote(
            part.at[t, 1 - core], got1.at[t], s1_ss.at[t], s1_rs.at[t], flipped(1)
        )
        copy.start()
        s1.append(copy)

    for t, b in enumerate(far):
        share(t, 2 * xor(high, b) + 1 - up)
    emit(dq, dq_out, scale)
    emit(dv, dv_out, 1.0)
    for t, b in enumerate(far):
        share(quarter + t, 2 * xor(high, b) + up)
        s1[t].wait_recv()
        send2[b] = (part[t, core] + got1[t]).astype(BF16)
        copy = remote(send2.at[b], got2.at[b], s2_ss.at[b], s2_rs.at[b], flipped(2))
        copy.start()
        s2.append(copy)
    for t, b in enumerate(far):
        s1[quarter + t].wait_recv()
        kept = part[quarter + t, core] + got1[quarter + t]
        s2[t].wait_recv()
        kept = kept + got2[b].astype(F32)
        if b == 0:
            wg_out[...] = kept
        else:
            send3[b] = kept.astype(BF16)
            copy = remote(send3.at[b], got3.at[b], s3_ss.at[b], s3_rs.at[b], flipped(4 * b))
            copy.start()
            s3.append(copy)

    dk[...] = dk[...] * scale
    for l in range(levels):

        @pl.when(sends_up(l))
        def _(l=l):
            dk_copies[l].wait_recv()
            dk[...] += dot_tn(pick[l], dkin[l])

    emit(dk, dk_out, 1.0)

    for b, copy in zip(reversed(range(1, quarter)), s3):
        copy.wait_recv()
        wg_out[...] += got3[b].astype(F32)
    for l in order:
        for copies in (slot_copies, dv_copies, dk_copies):
            pl.when(sends_down(l))(copies[l].wait_send)
        for copies in (k_copies, v_copies):
            pl.when(sends_up(l))(copies[l].wait_send)
    for copy in s1 + s2 + s3:
        copy.wait_send()


def finish(*refs):
    count = len(refs) // 2
    copies = [
        pltpu.make_async_copy(refs[i], refs[count + i], refs[-1].at[i]) for i in range(count)
    ]
    for copy in copies:
        copy.start()
    for copy in copies:
        copy.wait()


def per_device(queries, keys, values, attended, out_grad, log_sum, picked, layer_input):
    tok, heads, dh = queries.shape
    n = lax.axis_size("kv")
    levels = n.bit_length() - 1
    cols = heads * dh
    width = layer_input.shape[1]
    rb = width // n
    rows = (levels + 1 + 7) // 8 * 8
    hbm = pl.BlockSpec(memory_space=pltpu.HBM)
    vmem = pl.BlockSpec(memory_space=pltpu.VMEM)
    sems = pltpu.SemaphoreType.DMA
    level_buf = pltpu.VMEM((levels, COMPACT, cols), BF16)
    out = pl.pallas_call(
        functools.partial(body, n, levels, heads, dh),
        out_shape=[pltpu.VMEM((tok * heads, dh), F32)] * 3 + [pltpu.VMEM((rb, cols), F32)],
        in_specs=[hbm] * 8,
        out_specs=[vmem] * 4,
        scratch_shapes=[
            pltpu.SMEM(picked.shape, jnp.int32),
            pltpu.VMEM((heads, tok), F32),
            pltpu.VMEM((tok, cols), F32),
            pltpu.VMEM((tok, cols), F32),
            pltpu.VMEM((tok, cols), F32),
            pltpu.VMEM((5, tok, heads, dh), BF16),
        ]
        + [pltpu.VMEM((tok, cols), BF16)] * 5
        + [
            pltpu.VMEM((tok, width), BF16),
            pltpu.VMEM((width, tok), BF16),
            pltpu.VMEM((rows, tok), F32),
            pltpu.VMEM((levels, rows, tok), F32),
            pltpu.VMEM((levels, COMPACT, tok), BF16),
        ]
        + [level_buf] * 8
        + [
            pltpu.VMEM((levels, heads, COMPACT, tok), F32),
            pltpu.VMEM((n // 2, 2, rb, cols), F32),
            pltpu.VMEM((n // 2, rb, cols), F32),
            pltpu.VMEM((n // 4, rb, cols), BF16),
            pltpu.VMEM((n // 4, rb, cols), BF16),
            pltpu.VMEM((n // 4, rb, cols), BF16),
            pltpu.VMEM((n // 4, rb, cols), BF16),
            sems,
            sems,
            sems,
            sems((5,)),
        ]
        + [sems((levels,))] * 10
        + [sems((n // 2,))] * 2
        + [sems((n // 4,))] * 4,
        compiler_params=pltpu.CompilerParams(
            collective_id=0, has_side_effects=True
        ),
    )(picked, queries, keys, values, attended, out_grad, log_sum.T, layer_input)
    dq, dk, dv, wg = pl.pallas_call(
        finish,
        out_shape=[jax.ShapeDtypeStruct(o.shape, F32) for o in out],
        in_specs=[vmem] * 4,
        out_specs=[hbm] * 4,
        scratch_shapes=[sems((4,))],
    )(*(pltpu.with_memory_space_constraint(o, pltpu.VMEM) for o in out))
    return *(g.reshape(tok, heads, dh) for g in (dq, dk, dv)), wg


def solution(mesh):
    placed = (P("kv", "tp", None),) * 5 + (P("kv", "tp"), P("kv", None), P("kv", None))
    return jax.shard_map(
        per_device,
        mesh=mesh,
        in_specs=placed,
        out_specs=(P("kv", "tp", None), P("kv", "tp", None), P("kv", "tp", None), P("kv", "tp")),
        check_vma=False,
    )
```

```python
import functools

import jax
import jax.numpy as jnp
from jax import lax
from jax.experimental import pallas as pl
from jax.experimental.pallas import tpu as pltpu
from jax.sharding import PartitionSpec as P

QB = 128
KB = 32
PER_SPAN = 4
COMPACT = PER_SPAN * KB
CHUNKS = 8
F32 = jnp.float32
BF16 = jnp.bfloat16


def xor(value, bits):
    out = value
    for i in range(bits.bit_length()):
        if bits >> i & 1:
            out = out + (1 << i) - (2 << i) * lax.rem(value // (1 << i), 2)
    return out


def dot_nt(a, b):
    return lax.dot_general(a, b, (((1,), (1,)), ((), ())), preferred_element_type=F32)


def dot_tn(a, b):
    return lax.dot_general(a, b, (((0,), (0,)), ((), ())), preferred_element_type=F32)


def dot_nn(a, b):
    return lax.dot_general(a, b, (((1,), (0,)), ((), ())), preferred_element_type=F32)


def body(
    n, levels, heads, dh,
    picked_hbm, q_hbm, k_hbm, v_hbm, att_hbm, og_hbm, log_hbm, x_hbm,
    dq_out, dk_out, dv_out, wg_out,
    picked, log_sum, dq, dk, dv, wg, raw, q, k, v, att, og, x, xt, slot, slot_in, pick, ksend, kin, vsend, vin, dvsend, dvin, dksend, dkin,
    wts, part, got1, send2, got2, psend, pgot, asend, agot, bsend, bgot,
    x_sem, picked_sem, log_sem, raw_sem, slot_ss, slot_rs, k_ss, k_rs, v_ss, v_rs, dv_ss, dv_rs, dk_ss, dk_rs,
    s1_ss, s1_rs, s2_ss, s2_rs, p_ss, p_rs, a_ss, a_rs, b_ss, b_rs,
):
    me = lax.axis_index("kv")
    tok, cols = q.shape
    query_count = tok // QB
    span_blocks = tok // KB
    rows = slot.shape[0]
    scale = dh ** (-0.5)
    quarter = n // 4
    rb = wg_out.shape[0]
    top = levels - 1
    order = list(reversed(range(levels)))
    landing = order

    def to(offset):
        return {"kv": lax.rem(me + offset + n, n)}

    def flipped(bits):
        low = lax.rem(me, 4)
        if bits == 1:
            return {"kv": me + 1 - 2 * lax.rem(me, 2)}
        return {"kv": me + 2 - 4 * (low // 2)}

    def tower(at):
        return {"kv": at * 4 + lax.rem(me, 4)}

    def remote(src, dst, ss, rs, device):
        return pltpu.make_async_remote_copy(
            src_ref=src, dst_ref=dst, send_sem=ss, recv_sem=rs,
            device_id=device, device_id_type=pl.DeviceIdType.MESH,
        )

    load_picked = pltpu.make_async_copy(picked_hbm, picked, picked_sem)
    load_picked.start()
    barrier = pltpu.get_barrier_semaphore()
    greeted = [to(1 << l) for l in range(levels)] + [to(-(1 << l)) for l in range(levels)]
    high = me // 4
    greeted += [flipped(1), flipped(2)]
    greeted += [tower(lax.rem(high + b, quarter)) for b in range(1, quarter)]
    for device in greeted:
        pl.semaphore_signal(
            barrier, inc=1, device_id=device, device_id_type=pl.DeviceIdType.MESH
        )

    loads = {}
    for i, (src, dst) in enumerate(
        ((k_hbm, k), (v_hbm, v), (q_hbm, q), (og_hbm, og), (att_hbm, att))
    ):
        loads[i] = (pltpu.make_async_copy(src, raw.at[i], raw_sem.at[i]), dst)
        loads[i][0].start()

    def settle(i):
        copy, dst = loads[i]
        copy.wait()
        for h in range(heads):
            dst[:, h * dh : (h + 1) * dh] = raw[i, :, h, :]

    load_x = pltpu.make_async_copy(x_hbm, x, x_sem)
    load_x.start()
    load_log = pltpu.make_async_copy(log_hbm, log_sum, log_sem)
    load_log.start()
    row = lax.broadcasted_iota(jnp.int32, (rows, tok), 0)
    lane = lax.broadcasted_iota(jnp.int32, (rows, tok), 1)
    back = jnp.zeros((rows, tok), jnp.int32)
    for l in range(levels):
        back = jnp.where(row == l + 1, 1 << l, back)
    ids = jnp.where(row <= levels, (me - back) * span_blocks + lane // KB, -2)
    load_picked.wait()
    live = []
    for b in range(query_count):
        hit = jnp.zeros((rows, tok), jnp.int32)
        for s in range(picked.shape[1]):
            p = picked[b, s]
            hit = jnp.where(ids == jnp.where(p < 0, -(1 << 30), p), 1, hit)
        live.append(hit.astype(F32))
    need = functools.reduce(jnp.maximum, live)
    below = lax.broadcasted_iota(jnp.int32, (tok, tok), 0)
    above = lax.broadcasted_iota(jnp.int32, (tok, tok), 1)
    steps = jnp.where((below % KB == 0) & (below // KB < above // KB), 1.0, 0.0).astype(BF16)
    rank = dot_nn(need.astype(BF16), steps)
    slot[...] = jnp.where(need > 0, rank * KB + (lane % KB).astype(F32), -1.0)

    pl.semaphore_wait(barrier, len(greeted))

    def sends_up(l):
        return me + (1 << l) < n

    def sends_down(l):
        return me >= 1 << l

    slot_copies = {}
    for l in order:
        slot_copies[l] = remote(
            slot, slot_in.at[l], slot_ss.at[l], slot_rs.at[l], to(-(1 << l))
        )
        pl.when(sends_down(l))(slot_copies[l].start)

    k_copies, v_copies, dv_copies, dk_copies = {}, {}, {}, {}
    for l in order:
        k_copies[l] = remote(ksend.at[l], kin.at[l], k_ss.at[l], k_rs.at[l], to(1 << l))
    settle(0)
    settle(1)

    def one_hot(row_values):
        sub = lax.broadcasted_iota(jnp.int32, (COMPACT, tok), 0).astype(F32)
        return jnp.where(sub == row_values, 1.0, 0.0).astype(BF16)

    head = [slice(h * dh, (h + 1) * dh) for h in range(heads)]
    for l in order:
        v_copies[l] = remote(vsend.at[l], vin.at[l], v_ss.at[l], v_rs.at[l], to(1 << l))
        dv_copies[l] = remote(
            dvsend.at[l], dvin.at[l], dv_ss.at[l], dv_rs.at[l], to(-(1 << l))
        )
        dk_copies[l] = remote(
            dksend.at[l], dkin.at[l], dk_ss.at[l], dk_rs.at[l], to(-(1 << l))
        )
    for l in order:

        @pl.when(sends_up(l))
        def _(l=l):
            slot_copies[l].wait_recv()
            chosen = one_hot(slot_in[l, l + 1 : l + 2, :])
            pick[l] = chosen
            ksend[l] = dot_nn(chosen, k[...]).astype(BF16)
            k_copies[l].start()

    spot = lax.rem(me, 4)
    near = [spot >= 1 << l for l in range(2)]
    inside = [spot + (1 << l) < 4 for l in range(2)]

    def offer(l, ready):
        @pl.when(jnp.logical_and(sends_up(l), ready))
        def _():
            vsend[l] = dot_nn(pick[l], v[...]).astype(BF16)
            v_copies[l].start()

    for l in range(2):
        offer(l, inside[l])
    for i in range(2, 5):
        settle(i)
    dots = []
    for c in head:
        column = jnp.sum(og[:, c].astype(F32) * att[:, c].astype(F32), axis=1, keepdims=True)
        dots.append(jnp.transpose(jnp.broadcast_to(column, (tok, 128)))[0:1, :])
    load_log.wait()
    stored = [log_sum[h : h + 1, :] for h in range(heads)]

    def key_mask(chosen, r):
        pieces = []
        for m in live:
            column = dot_nt(chosen, m.astype(BF16))[:, r : r + 1]
            pieces.append(jnp.broadcast_to(column, (column.shape[0], QB)))
        return jnp.concatenate(pieces, axis=1) > 0

    own_mask = key_mask(jnp.where(below == above, 1.0, 0.0).astype(BF16), 0) & (below <= above)
    for h, c in enumerate(head):
        w = jnp.where(own_mask, jnp.exp(dot_nt(k[:, c], q[:, c]) * scale - stored[h]), 0.0)
        dv[:, c] = dot_nn(w.astype(BF16), og[:, c])
        g = (w * (dot_nt(v[:, c], og[:, c]) - dots[h])).astype(BF16)
        dk[:, c] = dot_nn(g, q[:, c])
        dq[:, c] = dot_tn(g, k[:, c])

    masks = {l: key_mask(one_hot(slot[l + 1 : l + 2, :]), l + 1) for l in order}
    load_x.wait()
    width = x.shape[1] // CHUNKS
    for i in range(CHUNKS):
        xt[i * width : (i + 1) * width, :] = jnp.transpose(x[:, i * width : (i + 1) * width])
    def meet(l, ready):
        @pl.when(jnp.logical_and(sends_down(l), ready))
        def _():
            k_copies[l].wait_recv()
            for h, c in enumerate(head):
                w = jnp.where(
                    masks[l], jnp.exp(dot_nt(kin[l, :, c], q[:, c]) * scale - stored[h]), 0.0
                )
                wts[l, h] = w
                dvsend[l, :, c] = dot_nn(w.astype(BF16), og[:, c]).astype(BF16)
            dv_copies[l].start()

    def emit(src, dst, factor):
        for h, c in enumerate(head):
            dst[pl.ds(h, tok, stride=heads), :] = src[:, c] * factor

    for l in range(2):
        meet(l, near[l])
    for l in order[: levels - 2]:
        meet(l, True)
    for l in (1, 0):
        meet(l, jnp.logical_not(near[l]))

    def finish_level(l, ready):
        @pl.when(jnp.logical_and(sends_down(l), ready))
        def _():
            v_copies[l].wait_recv()
            for h, c in enumerate(head):
                g = (wts[l, h] * (dot_nt(vin[l, :, c], og[:, c]) - dots[h])).astype(BF16)
                dksend[l, :, c] = (dot_nn(g, q[:, c]) * scale).astype(BF16)
                dq[:, c] += dot_tn(g, kin[l, :, c])
            dk_copies[l].start()

    for l in order:
        offer(l, jnp.logical_not(inside[l]) if l < 2 else True)
    for l in (1, 0):
        finish_level(l, near[l])
    for l in landing:

        @pl.when(sends_up(l))
        def _(l=l):
            dv_copies[l].wait_recv()
            dv[...] += dot_tn(pick[l], dvin[l])

    rounded = dv[...].astype(BF16)
    core = lax.rem(me, 2)
    up = lax.rem(me, 4) // 2
    odd = lax.rem(high, 2)
    pair = high // 2
    pairs = quarter // 2
    mate = 2 * pair + 1 - odd
    chunk = 2 * rb
    hr = rb // 2
    others = quarter - 2
    turns, passes = [], []
    for t in range(others):
        there = lax.rem(pair + pairs - t // 2 - 1, pairs)
        above = jnp.where(there > pair, 1, 0)
        turns.append(2 * there + (t % 2) * (1 - above) + (1 - t % 2) * above)
        passes.append(above != odd)
    def arrival(landed, sem, at, h):
        return remote(landed.at[at, h], landed.at[at, h], sem.at[at, h], sem.at[at, h], flipped(1))

    s1, s2, p_copies, a_copies, b_copies = {}, {}, {}, {}, {}

    def share(t, at, side):
        first = pl.multiple_of((2 * at + side) * chunk, chunk)
        w = dot_nn(xt[pl.ds(first, chunk), :], rounded)
        part[t] = w.reshape(2, rb, cols)
        s1[t] = remote(
            part.at[t, 1 - core], got1.at[t], s1_ss.at[t], s1_rs.at[t], flipped(1)
        )
        s1[t].start()

    def halves():
        return [(h, slice(h * hr, (h + 1) * hr)) for h in range(2)]

    for t in range(quarter):
        for h in range(2):
            s2[t, h] = remote(
                send2.at[t, h], got2.at[t, h], s2_ss.at[t, h], s2_rs.at[t, h], flipped(2)
            )
    for i in range(2):
        p_copies[i] = remote(psend.at[i], pgot.at[i], p_ss.at[i], p_rs.at[i], tower(mate))

    def cross(t, extra=None):
        s1[t].wait_recv()
        for h, span in halves():
            total = part[t, core, span, :] + got1[t, span, :]
            if extra is not None:
                total = total + extra[span, :].astype(F32)
            send2[t, h] = total.astype(BF16)
            s2[t, h].start()

    def pack(i, t):
        s1[t].wait_recv()
        psend[i] = (part[t, core] + got1[t]).astype(BF16)

    def relay(t):
        at = turns[t]
        s1[quarter + t].wait_recv()
        for h, span in halves():
            s2[t, h].wait_recv()
            kept = part[quarter + t, core, span, :] + got1[quarter + t, span, :]
            kept = kept + got2[t, h].astype(F32)
            a_copies[t, h] = remote(
                asend.at[t, h], agot.at[at, h], a_ss.at[t, h], a_rs.at[at, h], tower(mate)
            )
            b_copies[t, h] = remote(
                bsend.at[t, h], bgot.at[high, h], b_ss.at[t, h], b_rs.at[high, h], tower(at)
            )

            @pl.when(passes[t])
            def _(kept=kept):
                asend[t, h] = kept.astype(BF16)
                a_copies[t, h].start()

            @pl.when(jnp.logical_not(passes[t]))
            def _(kept=kept):
                arrival(agot, a_rs, at, h).wait_recv()
                bsend[t, h] = (kept + agot[at, h].astype(F32)).astype(BF16)
                b_copies[t, h].start()

    far, home = quarter - 1, 2 * quarter - 1
    sender = passes[0]
    joiner = jnp.logical_not(sender)
    eager = jnp.logical_and(joiner, odd == 1)
    patient = jnp.logical_and(joiner, odd == 0)
    out_copies = {
        h: remote(
            bsend.at[others, h], bgot.at[high, h],
            b_ss.at[others, h], b_rs.at[high, h], tower(mate),
        )
        for h in range(2)
    }

    def mate_out():
        s1[home - 1].wait_recv()
        for h, span in halves():
            s2[others, h].wait_recv()
            kept = part[home - 1, core, span, :] + got1[home - 1, span, :]
            bsend[others, h] = (kept + got2[others, h].astype(F32)).astype(BF16)
            out_copies[h].start()

    share(0, turns[0], 1 - up)
    share(others, mate, 1 - up)
    share(home - 1, mate, up)
    for t in range(1, others):
        share(t, turns[t], 1 - up)
    pl.when(eager)(lambda: cross(others))
    cross(0)

    @pl.when(sender)
    def _():
        pack(0, others)
        p_copies[0].start()
        pack(1, home - 1)

    for t in range(1, others):
        cross(t)
    pl.when(patient)(lambda: cross(others))
    for l in landing:
        finish_level(l, jnp.logical_and(joiner, jnp.logical_not(near[l])) if l < 2 else joiner)
    share(far, high, 1 - up)
    for t in range(others):
        share(quarter + t, turns[t], up)
    share(home, high, up)
    pl.when(eager)(mate_out)
    relay(0)
    pl.when(sender)(lambda: cross(far))

    @pl.when(joiner)
    def _():
        p_copies[0].wait_recv()
        cross(far, pgot.at[0])

    pl.when(patient)(mate_out)
    for t in range(1, others):
        relay(t)
    for l in landing:
        finish_level(l, jnp.logical_and(sender, jnp.logical_not(near[l])) if l < 2 else sender)
    pl.when(sender)(p_copies[1].start)
    emit(dq, dq_out, scale)
    emit(dv, dv_out, 1.0)
    dk[...] = dk[...] * scale
    for l in range(levels):

        @pl.when(sends_up(l))
        def _(l=l):
            dk_copies[l].wait_recv()
            dk[...] += dot_tn(pick[l], dkin[l])

    emit(dk, dk_out, 1.0)

    s1[home].wait_recv()
    for h, span in halves():
        s2[far, h].wait_recv()
        total = part[home, core, span, :] + got1[home, span, :]
        wg[span, :] = total + got2[far, h].astype(F32)

    @pl.when(joiner)
    def _():
        p_copies[1].wait_recv()
        wg[...] += pgot[1].astype(F32)

    for src in range(quarter):
        relays = jnp.where(src < high, src % 2, 1 - src % 2) == 1
        relays = jnp.where(src == mate, passes[0], relays)

        @pl.when(jnp.logical_and(src != high, relays))
        def _(src=src):
            for h, span in halves():
                arrival(bgot, b_rs, src, h).wait_recv()
                wg[span, :] += bgot[src, h].astype(F32)

    wg_out[...] = wg[...]
    for l in order:
        for copies in (slot_copies, dv_copies, dk_copies):
            pl.when(sends_down(l))(copies[l].wait_send)
        for copies in (k_copies, v_copies):
            pl.when(sends_up(l))(copies[l].wait_send)
    for copy in s1.values():
        copy.wait_send()
    for (t, h), copy in s2.items():
        if t == others:
            pl.when(joiner)(copy.wait_send)
        else:
            copy.wait_send()
    for i in range(2):
        pl.when(sender)(p_copies[i].wait_send)
        pl.when(joiner)(out_copies[i].wait_send)
    for (t, h), copy in a_copies.items():
        pl.when(passes[t])(copy.wait_send)
        pl.when(jnp.logical_not(passes[t]))(b_copies[t, h].wait_send)


def finish(*refs):
    count = len(refs) // 2
    copies = [
        pltpu.make_async_copy(refs[i], refs[count + i], refs[-1].at[i]) for i in range(count)
    ]
    for copy in copies:
        copy.start()
    for copy in copies:
        copy.wait()


def per_device(queries, keys, values, attended, out_grad, log_sum, picked, layer_input):
    tok, heads, dh = queries.shape
    n = lax.axis_size("kv")
    quarter = n // 4
    levels = n.bit_length() - 1
    cols = heads * dh
    width = layer_input.shape[1]
    rb = width // n
    rows = (levels + 1 + 7) // 8 * 8
    hbm = pl.BlockSpec(memory_space=pltpu.HBM)
    vmem = pl.BlockSpec(memory_space=pltpu.VMEM)
    sems = pltpu.SemaphoreType.DMA
    level_buf = pltpu.VMEM((levels, COMPACT, cols), BF16)
    out = pl.pallas_call(
        functools.partial(body, n, levels, heads, dh),
        out_shape=[pltpu.VMEM((tok * heads, dh), F32)] * 3 + [pltpu.VMEM((rb, cols), F32)],
        in_specs=[hbm] * 8,
        out_specs=[vmem] * 4,
        scratch_shapes=[
            pltpu.SMEM(picked.shape, jnp.int32),
            pltpu.VMEM((heads, tok), F32),
            pltpu.VMEM((tok, cols), F32),
            pltpu.VMEM((tok, cols), F32),
            pltpu.VMEM((tok, cols), F32),
            pltpu.VMEM((rb, cols), F32),
            pltpu.VMEM((5, tok, heads, dh), BF16),
        ]
        + [pltpu.VMEM((tok, cols), BF16)] * 5
        + [
            pltpu.VMEM((tok, width), BF16),
            pltpu.VMEM((width, tok), BF16),
            pltpu.VMEM((rows, tok), F32),
            pltpu.VMEM((levels, rows, tok), F32),
            pltpu.VMEM((levels, COMPACT, tok), BF16),
        ]
        + [level_buf] * 8
        + [
            pltpu.VMEM((levels, heads, COMPACT, tok), F32),
            pltpu.VMEM((n // 2, 2, rb, cols), F32),
            pltpu.VMEM((n // 2, rb, cols), F32),
            pltpu.VMEM((quarter, 2, rb // 2, cols), BF16),
            pltpu.VMEM((quarter, 2, rb // 2, cols), BF16),
            pltpu.VMEM((2, rb, cols), BF16),
            pltpu.VMEM((2, rb, cols), BF16),
        ]
        + [pltpu.VMEM((quarter, 2, rb // 2, cols), BF16)] * 4
        + [
            sems,
            sems,
            sems,
            sems((5,)),
        ]
        + [sems((levels,))] * 10
        + [sems((n // 2,))] * 2
        + [sems((quarter, 2))] * 2
        + [sems((2,))] * 2
        + [sems((quarter, 2))] * 4,
        compiler_params=pltpu.CompilerParams(
            collective_id=0, has_side_effects=True
        ),
    )(picked, queries, keys, values, attended, out_grad, log_sum.T, layer_input)
    dq, dk, dv, wg = pl.pallas_call(
        finish,
        out_shape=[jax.ShapeDtypeStruct(o.shape, F32) for o in out],
        in_specs=[vmem] * 4,
        out_specs=[hbm] * 4,
        scratch_shapes=[sems((4,))],
    )(*(pltpu.with_memory_space_constraint(o, pltpu.VMEM) for o in out))
    return *(g.reshape(tok, heads, dh) for g in (dq, dk, dv)), wg


def solution(mesh):
    placed = (P("kv", "tp", None),) * 5 + (P("kv", "tp"), P("kv", None), P("kv", None))
    return jax.shard_map(
        per_device,
        mesh=mesh,
        in_specs=placed,
        out_specs=(P("kv", "tp", None), P("kv", "tp", None), P("kv", "tp", None), P("kv", "tp")),
        check_vma=False,
    )
```

```python
import functools

import jax
import jax.numpy as jnp
from jax import lax
from jax.experimental import pallas as pl
from jax.experimental.pallas import tpu as pltpu
from jax.sharding import PartitionSpec as P

QB = 128
KB = 32
PER_SPAN = 4
COMPACT = PER_SPAN * KB
CHUNKS = 8
PIECES = 4
F32 = jnp.float32
BF16 = jnp.bfloat16


def xor(value, bits):
    out = value
    for i in range(bits.bit_length()):
        if bits >> i & 1:
            out = out + (1 << i) - (2 << i) * lax.rem(value // (1 << i), 2)
    return out


def dot_nt(a, b):
    return lax.dot_general(a, b, (((1,), (1,)), ((), ())), preferred_element_type=F32)


def dot_tn(a, b):
    return lax.dot_general(a, b, (((0,), (0,)), ((), ())), preferred_element_type=F32)


def dot_nn(a, b):
    return lax.dot_general(a, b, (((1,), (0,)), ((), ())), preferred_element_type=F32)


def body(
    n, levels, heads, dh,
    picked_hbm, q_hbm, k_hbm, v_hbm, att_hbm, og_hbm, log_hbm, x_hbm,
    dq_out, dk_out, dv_out, wg_out,
    picked, log_sum, dq, dk, dv, wg, raw, q, k, v, att, og, x, xt, slot, slot_in, pick, kvsend, kin, vin, dsend, dvin, dkin,
    wts, part, got1, send2, got2, psend, pgot, zsend, agot, bgot,
    x_sem, picked_sem, log_sem, raw_sem, up_ss, down_ss, slot_rs, k_rs, v_rs, dv_rs, dk_rs,
    s1_ss, s1_rs, s2_ss, s2_rs, p_ss, p_rs, z_ss, a_rs, b_rs,
):
    me = lax.axis_index("kv")
    tok, cols = q.shape
    query_count = tok // QB
    span_blocks = tok // KB
    rows = slot.shape[0]
    scale = dh ** (-0.5)
    quarter = n // 4
    rb = wg_out.shape[0]
    top = levels - 1
    order = list(reversed(range(levels)))
    landing = order

    def to(offset):
        return {"kv": lax.rem(me + offset + n, n)}

    def flipped(bits):
        low = lax.rem(me, 4)
        if bits == 1:
            return {"kv": me + 1 - 2 * lax.rem(me, 2)}
        return {"kv": me + 2 - 4 * (low // 2)}

    def tower(at):
        return {"kv": at * 4 + lax.rem(me, 4)}

    def remote(src, dst, ss, rs, device):
        return pltpu.make_async_remote_copy(
            src_ref=src, dst_ref=dst, send_sem=ss, recv_sem=rs,
            device_id=device, device_id_type=pl.DeviceIdType.MESH,
        )

    load_picked = pltpu.make_async_copy(picked_hbm, picked, picked_sem)
    load_picked.start()
    barrier = pltpu.get_barrier_semaphore()
    greeted = [to(1 << l) for l in range(levels)] + [to(-(1 << l)) for l in range(levels)]
    high = me // 4
    greeted += [flipped(1), flipped(2)]
    greeted += [tower(lax.rem(high + b, quarter)) for b in range(1, quarter)]
    for device in greeted:
        pl.semaphore_signal(
            barrier, inc=1, device_id=device, device_id_type=pl.DeviceIdType.MESH
        )

    loads = {}
    for i, (src, dst) in enumerate(
        ((k_hbm, k), (v_hbm, v), (q_hbm, q), (og_hbm, og), (att_hbm, att))
    ):
        loads[i] = (pltpu.make_async_copy(src, raw.at[i], raw_sem.at[i]), dst)
        loads[i][0].start()

    def settle(i):
        copy, dst = loads[i]
        copy.wait()
        for h in range(heads):
            dst[:, h * dh : (h + 1) * dh] = raw[i, :, h, :]

    load_x = pltpu.make_async_copy(x_hbm, x, x_sem)
    load_x.start()
    load_log = pltpu.make_async_copy(log_hbm, log_sum, log_sem)
    load_log.start()
    row = lax.broadcasted_iota(jnp.int32, (rows, tok), 0)
    lane = lax.broadcasted_iota(jnp.int32, (rows, tok), 1)
    back = jnp.zeros((rows, tok), jnp.int32)
    for l in range(levels):
        back = jnp.where(row == l + 1, 1 << l, back)
    ids = jnp.where(row <= levels, (me - back) * span_blocks + lane // KB, -2)
    load_picked.wait()
    live = []
    for b in range(query_count):
        hit = jnp.zeros((rows, tok), jnp.int32)
        for s in range(picked.shape[1]):
            p = picked[b, s]
            hit = jnp.where(ids == jnp.where(p < 0, -(1 << 30), p), 1, hit)
        live.append(hit.astype(F32))
    need = functools.reduce(jnp.maximum, live)
    below = lax.broadcasted_iota(jnp.int32, (tok, tok), 0)
    above = lax.broadcasted_iota(jnp.int32, (tok, tok), 1)
    steps = jnp.where((below % KB == 0) & (below // KB < above // KB), 1.0, 0.0).astype(BF16)
    rank = dot_nn(need.astype(BF16), steps)
    slot[...] = jnp.where(need > 0, rank * KB + (lane % KB).astype(F32), -1.0)

    pl.semaphore_wait(barrier, len(greeted))

    def sends_up(l):
        return me + (1 << l) < n

    def sends_down(l):
        return me >= 1 << l

    slot_copies = {}
    for l in order:
        slot_copies[l] = remote(
            slot, slot_in.at[l], down_ss.at[l], slot_rs.at[l], to(-(1 << l))
        )
        pl.when(sends_down(l))(slot_copies[l].start)

    k_copies, v_copies, dv_copies, dk_copies = {}, {}, {}, {}
    for l in order:
        k_copies[l] = remote(
            kvsend.at[l, 0], kin.at[l], up_ss.at[l], k_rs.at[l], to(1 << l)
        )
    settle(0)
    settle(1)

    def one_hot(row_values):
        sub = lax.broadcasted_iota(jnp.int32, (COMPACT, tok), 0).astype(F32)
        return jnp.where(sub == row_values, 1.0, 0.0).astype(BF16)

    head = [slice(h * dh, (h + 1) * dh) for h in range(heads)]
    for l in order:
        v_copies[l] = remote(
            kvsend.at[l, 1], vin.at[l], up_ss.at[l], v_rs.at[l], to(1 << l)
        )
        dv_copies[l] = remote(
            dsend.at[l, :COMPACT], dvin.at[l], down_ss.at[l], dv_rs.at[l], to(-(1 << l))
        )
        dk_copies[l] = remote(
            dsend.at[l, COMPACT : 2 * COMPACT], dkin.at[l], down_ss.at[l], dk_rs.at[l],
            to(-(1 << l)),
        )
    for l in order[: levels - 2] + [0, 1]:

        @pl.when(sends_up(l))
        def _(l=l):
            slot_copies[l].wait_recv()
            chosen = one_hot(slot_in[l, l + 1 : l + 2, :])
            kvsend[l, 0] = dot_nn(chosen, k[...]).astype(BF16)
            k_copies[l].start()
            pick[l] = jnp.transpose(chosen)
            kvsend[l, 1] = dot_nn(chosen, v[...]).astype(BF16)

    spot = lax.rem(me, 4)
    near = [spot >= 1 << l for l in range(2)]
    inside = [spot + (1 << l) < 4 for l in range(2)]

    def offer(l, ready):
        @pl.when(jnp.logical_and(sends_up(l), ready))
        def _():
            v_copies[l].start()

    for l in range(2):
        offer(l, inside[l])
    for i in range(2, 5):
        settle(i)
    dots = []
    for c in head:
        column = jnp.sum(og[:, c].astype(F32) * att[:, c].astype(F32), axis=1, keepdims=True)
        dots.append(jnp.transpose(jnp.broadcast_to(column, (tok, 128)))[0:1, :])
    load_log.wait()
    stored = [log_sum[h : h + 1, :] for h in range(heads)]

    def key_mask(chosen, r):
        pieces = []
        for m in live:
            column = dot_nt(chosen, m.astype(BF16))[:, r : r + 1]
            pieces.append(jnp.broadcast_to(column, (column.shape[0], QB)))
        return jnp.concatenate(pieces, axis=1) > 0

    own_mask = key_mask(jnp.where(below == above, 1.0, 0.0).astype(BF16), 0) & (below <= above)
    for h, c in enumerate(head):
        w = jnp.where(own_mask, jnp.exp(dot_nt(k[:, c], q[:, c]) * scale - stored[h]), 0.0)
        dv[:, c] = dot_nn(w.astype(BF16), og[:, c])
        g = (w * (dot_nt(v[:, c], og[:, c]) - dots[h])).astype(BF16)
        dk[:, c] = dot_nn(g, q[:, c])
        dq[:, c] = dot_tn(g, k[:, c])

    masks = {l: key_mask(one_hot(slot[l + 1 : l + 2, :]), l + 1) for l in order}
    load_x.wait()
    width = x.shape[1] // CHUNKS
    for i in range(CHUNKS):
        xt[i * width : (i + 1) * width, :] = jnp.transpose(x[:, i * width : (i + 1) * width])
    def meet(l, ready):
        @pl.when(jnp.logical_and(sends_down(l), ready))
        def _():
            k_copies[l].wait_recv()
            for h, c in enumerate(head):
                w = jnp.where(
                    masks[l], jnp.exp(dot_nt(kin[l, :, c], q[:, c]) * scale - stored[h]), 0.0
                )
                wts[l, h] = w
                dsend[l, :COMPACT, c] = dot_nn(w.astype(BF16), og[:, c]).astype(BF16)
            dv_copies[l].start()

    def emit(src, dst, factor):
        for h, c in enumerate(head):
            dst[pl.ds(h, tok, stride=heads), :] = src[:, c] * factor

    for l in range(2):
        meet(l, near[l])
    for l in order[: levels - 2]:
        meet(l, True)
    for l in (1, 0):
        meet(l, jnp.logical_not(near[l]))

    def finish_level(l, ready):
        @pl.when(jnp.logical_and(sends_down(l), ready))
        def _():
            v_copies[l].wait_recv()
            for h, c in enumerate(head):
                g = (wts[l, h] * (dot_nt(vin[l, :, c], og[:, c]) - dots[h])).astype(BF16)
                dsend[l, COMPACT : 2 * COMPACT, c] = (dot_nn(g, q[:, c]) * scale).astype(BF16)
                dq[:, c] += dot_tn(g, kin[l, :, c])
            dk_copies[l].start()

    for l in order:
        offer(l, jnp.logical_not(inside[l]) if l < 2 else True)
    for l in (1, 0):
        finish_level(l, near[l])
    first = [me // 4 - (1 << l) // 4 == 0 for l in range(levels)]
    for l in order[: levels - 2]:
        finish_level(l, first[l])
    for l in landing:

        @pl.when(sends_up(l))
        def _(l=l):
            dv_copies[l].wait_recv()
            dv[...] += dot_nn(pick[l], dvin[l])

    rounded = dv[...].astype(BF16)
    core = lax.rem(me, 2)
    up = lax.rem(me, 4) // 2
    odd = lax.rem(high, 2)
    pair = high // 2
    pairs = quarter // 2
    mate = 2 * pair + 1 - odd
    chunk = 2 * rb
    pieces = send2.shape[1]
    hr = rb // pieces
    others = quarter - 2
    turns, passes = [], []
    for t in range(others):
        there = lax.rem(pair + pairs - t // 2 - 1, pairs)
        above = jnp.where(there > pair, 1, 0)
        turns.append(2 * there + (t % 2) * (1 - above) + (1 - t % 2) * above)
        passes.append(above != odd)
    s1, s2, p_copies, a_copies, b_copies = {}, {}, {}, {}, {}

    def share(t, at, side):
        first = pl.multiple_of((2 * at + side) * chunk, chunk)
        w = dot_nn(xt[pl.ds(first, chunk), :], rounded)
        part[t] = w.reshape(2, rb, cols)
        s1[t] = remote(
            part.at[t, 1 - core], got1.at[t], s1_ss, s1_rs.at[t], flipped(1)
        )
        s1[t].start()

    def halves():
        return [(h, slice(h * hr, (h + 1) * hr)) for h in range(pieces)]

    for t in range(quarter):
        for h in range(pieces):
            s2[t, h] = remote(
                send2.at[t, h], got2.at[t, h], s2_ss.at[t], s2_rs.at[t, h], flipped(2)
            )
    for i in range(2):
        p_copies[i] = remote(psend.at[i], pgot.at[i], p_ss, p_rs.at[i], tower(mate))

    def cross(t, extra=None):
        s1[t].wait_recv()
        for h, span in halves():
            total = part[t, core, span, :] + got1[t, span, :]
            if extra is not None:
                total = total + extra[span, :].astype(F32)
            send2[t, h] = total.astype(BF16)
            s2[t, h].start()

    def pack(i, t):
        s1[t].wait_recv()
        psend[i] = (part[t, core] + got1[t]).astype(BF16)

    def relay(t):
        at = turns[t]
        s1[quarter + t].wait_recv()
        for h, span in halves():
            s2[t, h].wait_recv()
            kept = part[quarter + t, core, span, :] + got1[quarter + t, span, :]
            kept = kept + got2[t, h].astype(F32)
            a_copies[t, h] = remote(
                zsend.at[t, h], agot.at[t, h], z_ss.at[t], a_rs.at[t, h], tower(mate)
            )
            b_copies[t, h] = remote(
                zsend.at[t, h], bgot.at[t // 2, h], z_ss.at[t], b_rs.at[t // 2, h], tower(at)
            )

            @pl.when(passes[t])
            def _(kept=kept):
                zsend[t, h] = kept.astype(BF16)
                a_copies[t, h].start()

            @pl.when(jnp.logical_not(passes[t]))
            def _(kept=kept):
                a_copies[t, h].wait_recv()
                zsend[t, h] = (kept + agot[t, h].astype(F32)).astype(BF16)
                b_copies[t, h].start()

    far, home = quarter - 1, 2 * quarter - 1
    sender = passes[0]
    joiner = jnp.logical_not(sender)
    eager = jnp.logical_and(joiner, odd == 1)
    gives = jnp.logical_not(eager)
    takes = jnp.logical_not(jnp.logical_and(sender, odd == 0))
    out_copies = {
        h: remote(
            zsend.at[others, h], bgot.at[pairs - 1, h],
            z_ss.at[others], b_rs.at[pairs - 1, h], tower(mate),
        )
        for h in range(pieces)
    }

    def mate_out():
        s1[home - 1].wait_recv()
        for h, span in halves():
            s2[others, h].wait_recv()
            kept = part[home - 1, core, span, :] + got1[home - 1, span, :]
            zsend[others, h] = (kept + got2[others, h].astype(F32)).astype(BF16)
            out_copies[h].start()

    share(0, turns[0], 1 - up)
    share(others, mate, 1 - up)
    share(home - 1, mate, up)
    for t in range(1, others):
        share(t, turns[t], 1 - up)
    cross(0)
    pl.when(eager)(lambda: cross(others))

    @pl.when(gives)
    def _():
        pack(0, others)
        p_copies[0].start()
        pack(1, home - 1)

    for t in range(1, others):
        cross(t)
    for l in landing:
        finish_level(l, jnp.logical_and(joiner, jnp.logical_not((near if l < 2 else first)[l])))
    share(far, high, 1 - up)
    for t in range(others):
        share(quarter + t, turns[t], up)
    share(home, high, up)
    relay(0)
    pl.when(eager)(mate_out)
    pl.when(jnp.logical_not(takes))(lambda: cross(far))

    def cross_home():
        p_copies[0].wait_recv()
        cross(far, pgot.at[0])

    pl.when(joiner)(cross_home)

    for t in range(1, others):
        relay(t)
    pl.when(jnp.logical_and(sender, takes))(cross_home)
    for l in landing:
        finish_level(l, jnp.logical_and(sender, jnp.logical_not((near if l < 2 else first)[l])))
    pl.when(gives)(p_copies[1].start)
    emit(dq, dq_out, scale)
    emit(dv, dv_out, 1.0)
    dk[...] = dk[...] * scale
    for l in range(levels):

        @pl.when(sends_up(l))
        def _(l=l):
            dk_copies[l].wait_recv()
            dk[...] += dot_nn(pick[l], dkin[l])

    emit(dk, dk_out, 1.0)

    s1[home].wait_recv()
    for h, span in halves():
        s2[far, h].wait_recv()
        total = part[home, core, span, :] + got1[home, span, :]
        wg[span, :] = total + got2[far, h].astype(F32)

    @pl.when(takes)
    def _():
        p_copies[1].wait_recv()
        wg[...] += pgot[1].astype(F32)

    def absorb(i):
        for h, span in halves():
            remote(
                zsend.at[i, h], bgot.at[i, h], z_ss.at[i], b_rs.at[i, h], tower(mate)
            ).wait_recv()
            wg[span, :] += bgot[i, h].astype(F32)

    pl.when(jnp.logical_not(takes))(lambda: absorb(pairs - 1))
    for i in range(pairs - 1):
        absorb(i)

    wg_out[...] = wg[...]
    for l in order:
        fed = remote(kvsend.at[l], kvsend.at[l], up_ss.at[l], k_rs.at[l], to(1 << l))
        pl.when(sends_up(l))(fed.wait_send)
        fed = remote(dsend.at[l], dsend.at[l], down_ss.at[l], dv_rs.at[l], to(-(1 << l)))
        pl.when(sends_down(l))(fed.wait_send)
    remote(part.at[:, 0], got1, s1_ss, s1_rs.at[0], flipped(1)).wait_send()
    for t in range(quarter):
        sent = remote(send2.at[t], got2.at[t], s2_ss.at[t], s2_rs.at[t, 0], flipped(2))
        pl.when(eager if t == others else True)(sent.wait_send)
    for t in range(others + 1):
        sent = remote(zsend.at[t], zsend.at[t], z_ss.at[t], a_rs.at[0, 0], tower(mate))
        pl.when(eager if t == others else True)(sent.wait_send)
    pl.when(gives)(remote(psend, pgot, p_ss, p_rs.at[0], tower(mate)).wait_send)


def finish(*refs):
    count = len(refs) // 2
    copies = [
        pltpu.make_async_copy(refs[i], refs[count + i], refs[-1].at[i]) for i in range(count)
    ]
    for copy in copies:
        copy.start()
    for copy in copies:
        copy.wait()


def per_device(queries, keys, values, attended, out_grad, log_sum, picked, layer_input):
    tok, heads, dh = queries.shape
    n = lax.axis_size("kv")
    quarter = n // 4
    levels = n.bit_length() - 1
    cols = heads * dh
    width = layer_input.shape[1]
    rb = width // n
    pieces = min(PIECES, rb // 8)
    rows = (levels + 1 + 7) // 8 * 8
    hbm = pl.BlockSpec(memory_space=pltpu.HBM)
    vmem = pl.BlockSpec(memory_space=pltpu.VMEM)
    sems = pltpu.SemaphoreType.DMA
    level_buf = pltpu.VMEM((levels, COMPACT, cols), BF16)
    out = pl.pallas_call(
        functools.partial(body, n, levels, heads, dh),
        out_shape=[pltpu.VMEM((tok * heads, dh), F32)] * 3 + [pltpu.VMEM((rb, cols), F32)],
        in_specs=[hbm] * 8,
        out_specs=[vmem] * 4,
        scratch_shapes=[
            pltpu.SMEM(picked.shape, jnp.int32),
            pltpu.VMEM((heads, tok), F32),
            pltpu.VMEM((tok, cols), F32),
            pltpu.VMEM((tok, cols), F32),
            pltpu.VMEM((tok, cols), F32),
            pltpu.VMEM((rb, cols), F32),
            pltpu.VMEM((5, tok, heads, dh), BF16),
        ]
        + [pltpu.VMEM((tok, cols), BF16)] * 5
        + [
            pltpu.VMEM((tok, width), BF16),
            pltpu.VMEM((width, tok), BF16),
            pltpu.VMEM((rows, tok), F32),
            pltpu.VMEM((levels, rows, tok), F32),
            pltpu.VMEM((levels, tok, COMPACT), BF16),
        ]
        + [pltpu.VMEM((levels, 2, COMPACT, cols), BF16), level_buf, level_buf]
        + [pltpu.VMEM((levels, 2 * COMPACT + 2 * rows * tok // cols, cols), BF16)]
        + [level_buf] * 2
        + [
            pltpu.VMEM((levels, heads, COMPACT, tok), F32),
            pltpu.VMEM((n // 2, 2, rb, cols), F32),
            pltpu.VMEM((n // 2, rb, cols), F32),
            pltpu.VMEM((quarter, pieces, rb // pieces, cols), BF16),
            pltpu.VMEM((quarter, pieces, rb // pieces, cols), BF16),
            pltpu.VMEM((2, rb, cols), BF16),
            pltpu.VMEM((2, rb, cols), BF16),
            pltpu.VMEM((quarter - 1, pieces, rb // pieces, cols), BF16),
            pltpu.VMEM((quarter - 2, pieces, rb // pieces, cols), BF16),
            pltpu.VMEM((quarter // 2, pieces, rb // pieces, cols), BF16),
            sems,
            sems,
            sems,
            sems((5,)),
        ]
        + [sems((levels,))] * 7
        + [
            sems,
            sems((n // 2,)),
            sems((quarter,)),
            sems((quarter, pieces)),
            sems,
            sems((2,)),
            sems((quarter - 1,)),
            sems((quarter - 2, pieces)),
            sems((quarter // 2, pieces)),
        ],
        compiler_params=pltpu.CompilerParams(
            collective_id=0, has_side_effects=True
        ),
    )(picked, queries, keys, values, attended, out_grad, log_sum.T, layer_input)
    dq, dk, dv, wg = pl.pallas_call(
        finish,
        out_shape=[jax.ShapeDtypeStruct(o.shape, F32) for o in out],
        in_specs=[vmem] * 4,
        out_specs=[hbm] * 4,
        scratch_shapes=[sems((4,))],
    )(*(pltpu.with_memory_space_constraint(o, pltpu.VMEM) for o in out))
    return *(g.reshape(tok, heads, dh) for g in (dq, dk, dv)), wg


def solution(mesh):
    placed = (P("kv", "tp", None),) * 5 + (P("kv", "tp"), P("kv", None), P("kv", None))
    return jax.shard_map(
        per_device,
        mesh=mesh,
        in_specs=placed,
        out_specs=(P("kv", "tp", None), P("kv", "tp", None), P("kv", "tp", None), P("kv", "tp")),
        check_vma=False,
    )
```

```python
import functools

import jax
import jax.numpy as jnp
from jax import lax
from jax.experimental import pallas as pl
from jax.experimental.pallas import tpu as pltpu
from jax.sharding import PartitionSpec as P

QB = 128
KB = 32
PER_SPAN = 4
COMPACT = PER_SPAN * KB
CHUNKS = 8
PIECES = 4
F32 = jnp.float32
BF16 = jnp.bfloat16


def xor(value, bits):
    out = value
    for i in range(bits.bit_length()):
        if bits >> i & 1:
            out = out + (1 << i) - (2 << i) * lax.rem(value // (1 << i), 2)
    return out


def dot_nt(a, b):
    return lax.dot_general(a, b, (((1,), (1,)), ((), ())), preferred_element_type=F32)


def dot_tn(a, b):
    return lax.dot_general(a, b, (((0,), (0,)), ((), ())), preferred_element_type=F32)


def dot_nn(a, b):
    return lax.dot_general(a, b, (((1,), (0,)), ((), ())), preferred_element_type=F32)


def body(
    n, levels, heads, dh,
    picked_hbm, q_hbm, k_hbm, v_hbm, att_hbm, og_hbm, log_hbm, x_hbm,
    dq_out, dk_out, dv_out, wg,
    picked, log_sum, dq, dk, dv, raw, q, k, v, att, og, x, xt, slot, slot_in, pick, kvsend, kin, vin, dsend, dvin, dkin,
    wts, part, got1, send2, got2, psend, pgot, zsend, agot, bgot,
    x_sem, picked_sem, log_sem, raw_sem, up_ss, down_ss, slot_rs, k_rs, v_rs, dv_rs, dk_rs,
    s1_ss, s1_rs, s2_ss, s2_rs, p_ss, p_rs, z_ss, a_rs, b_rs,
):
    me = lax.axis_index("kv")
    tok, cols = q.shape
    query_count = tok // QB
    span_blocks = tok // KB
    rows = slot.shape[0]
    scale = dh ** (-0.5)
    quarter = n // 4
    rb = wg.shape[0]
    top = levels - 1
    order = list(reversed(range(levels)))
    landing = order

    def to(offset):
        return {"kv": lax.rem(me + offset + n, n)}

    def flipped(bits):
        low = lax.rem(me, 4)
        if bits == 1:
            return {"kv": me + 1 - 2 * lax.rem(me, 2)}
        return {"kv": me + 2 - 4 * (low // 2)}

    def tower(at):
        return {"kv": at * 4 + lax.rem(me, 4)}

    def remote(src, dst, ss, rs, device):
        return pltpu.make_async_remote_copy(
            src_ref=src, dst_ref=dst, send_sem=ss, recv_sem=rs,
            device_id=device, device_id_type=pl.DeviceIdType.MESH,
        )

    load_picked = pltpu.make_async_copy(picked_hbm, picked, picked_sem)
    load_picked.start()
    barrier = pltpu.get_barrier_semaphore()
    greeted = [to(1 << l) for l in range(levels)] + [to(-(1 << l)) for l in range(levels)]
    high = me // 4
    greeted += [flipped(1), flipped(2)]
    greeted += [tower(lax.rem(high + b, quarter)) for b in range(1, quarter)]
    for device in greeted:
        pl.semaphore_signal(
            barrier, inc=1, device_id=device, device_id_type=pl.DeviceIdType.MESH
        )

    loads = {}
    for i, (src, dst) in enumerate(
        ((k_hbm, k), (v_hbm, v), (q_hbm, q), (og_hbm, og), (att_hbm, att))
    ):
        loads[i] = (pltpu.make_async_copy(src, raw.at[i], raw_sem.at[i]), dst)
        loads[i][0].start()

    def settle(i):
        copy, dst = loads[i]
        copy.wait()
        for h in range(heads):
            dst[:, h * dh : (h + 1) * dh] = raw[i, :, h, :]

    load_x = pltpu.make_async_copy(x_hbm, x, x_sem)
    load_x.start()
    load_log = pltpu.make_async_copy(log_hbm, log_sum, log_sem)
    load_log.start()
    row = lax.broadcasted_iota(jnp.int32, (rows, tok), 0)
    lane = lax.broadcasted_iota(jnp.int32, (rows, tok), 1)
    back = jnp.zeros((rows, tok), jnp.int32)
    for l in range(levels):
        back = jnp.where(row == l + 1, 1 << l, back)
    ids = jnp.where(row <= levels, (me - back) * span_blocks + lane // KB, -2)
    load_picked.wait()
    live = []
    for b in range(query_count):
        hit = jnp.zeros((rows, tok), jnp.int32)
        for s in range(picked.shape[1]):
            p = picked[b, s]
            hit = jnp.where(ids == jnp.where(p < 0, -(1 << 30), p), 1, hit)
        live.append(hit.astype(F32))
    need = functools.reduce(jnp.maximum, live)
    below = lax.broadcasted_iota(jnp.int32, (tok, tok), 0)
    above = lax.broadcasted_iota(jnp.int32, (tok, tok), 1)
    steps = jnp.where((below % KB == 0) & (below // KB < above // KB), 1.0, 0.0).astype(BF16)
    rank = dot_nn(need.astype(BF16), steps)
    slot[...] = jnp.where(need > 0, rank * KB + (lane % KB).astype(F32), -1.0)

    pl.semaphore_wait(barrier, len(greeted))

    def sends_up(l):
        return me + (1 << l) < n

    def sends_down(l):
        return me >= 1 << l

    slot_copies = {}
    for l in order:
        slot_copies[l] = remote(
            slot, slot_in.at[l], down_ss.at[l], slot_rs.at[l], to(-(1 << l))
        )
        pl.when(sends_down(l))(slot_copies[l].start)

    k_copies, v_copies, dv_copies, dk_copies = {}, {}, {}, {}
    for l in order:
        k_copies[l] = remote(
            kvsend.at[l, 0], kin.at[l], up_ss.at[l], k_rs.at[l], to(1 << l)
        )
    settle(0)
    settle(1)

    def one_hot(row_values):
        sub = lax.broadcasted_iota(jnp.int32, (COMPACT, tok), 0).astype(F32)
        return jnp.where(sub == row_values, 1.0, 0.0).astype(BF16)

    head = [slice(h * dh, (h + 1) * dh) for h in range(heads)]
    for l in order:
        v_copies[l] = remote(
            kvsend.at[l, 1], vin.at[l], up_ss.at[l], v_rs.at[l], to(1 << l)
        )
        dv_copies[l] = remote(
            dsend.at[l, :COMPACT], dvin.at[l], down_ss.at[l], dv_rs.at[l], to(-(1 << l))
        )
        dk_copies[l] = remote(
            dsend.at[l, COMPACT : 2 * COMPACT], dkin.at[l], down_ss.at[l], dk_rs.at[l],
            to(-(1 << l)),
        )
    for l in order[: levels - 2] + [0, 1]:

        @pl.when(sends_up(l))
        def _(l=l):
            slot_copies[l].wait_recv()
            chosen = one_hot(slot_in[l, l + 1 : l + 2, :])
            kvsend[l, 0] = dot_nn(chosen, k[...]).astype(BF16)
            k_copies[l].start()
            pick[l] = jnp.transpose(chosen)
            kvsend[l, 1] = dot_nn(chosen, v[...]).astype(BF16)

    spot = lax.rem(me, 4)
    near = [spot >= 1 << l for l in range(2)]
    inside = [spot + (1 << l) < 4 for l in range(2)]

    def offer(l, ready):
        @pl.when(jnp.logical_and(sends_up(l), ready))
        def _():
            v_copies[l].start()

    for l in range(2):
        offer(l, inside[l])
    for i in range(2, 5):
        settle(i)
    dots = []
    for c in head:
        column = jnp.sum(og[:, c].astype(F32) * att[:, c].astype(F32), axis=1, keepdims=True)
        dots.append(jnp.transpose(jnp.broadcast_to(column, (tok, 128)))[0:1, :])
    load_log.wait()
    stored = [log_sum[h : h + 1, :] for h in range(heads)]

    def key_mask(chosen, r):
        pieces = []
        for m in live:
            column = dot_nt(chosen, m.astype(BF16))[:, r : r + 1]
            pieces.append(jnp.broadcast_to(column, (column.shape[0], QB)))
        return jnp.concatenate(pieces, axis=1) > 0

    own_mask = key_mask(jnp.where(below == above, 1.0, 0.0).astype(BF16), 0) & (below <= above)
    for h, c in enumerate(head):
        w = jnp.where(own_mask, jnp.exp(dot_nt(k[:, c], q[:, c]) * scale - stored[h]), 0.0)
        dv[:, c] = dot_nn(w.astype(BF16), og[:, c])
        g = (w * (dot_nt(v[:, c], og[:, c]) - dots[h])).astype(BF16)
        dk[:, c] = dot_nn(g, q[:, c])
        dq[:, c] = dot_tn(g, k[:, c])

    masks = {l: key_mask(one_hot(slot[l + 1 : l + 2, :]), l + 1) for l in order}
    load_x.wait()
    width = x.shape[1] // CHUNKS
    for i in range(CHUNKS):
        xt[i * width : (i + 1) * width, :] = jnp.transpose(x[:, i * width : (i + 1) * width])
    def meet(l, ready):
        @pl.when(jnp.logical_and(sends_down(l), ready))
        def _():
            k_copies[l].wait_recv()
            for h, c in enumerate(head):
                w = jnp.where(
                    masks[l], jnp.exp(dot_nt(kin[l, :, c], q[:, c]) * scale - stored[h]), 0.0
                )
                wts[l, h] = w
                dsend[l, :COMPACT, c] = dot_nn(w.astype(BF16), og[:, c]).astype(BF16)
            dv_copies[l].start()

    def emit(src, dst, factor):
        for h, c in enumerate(head):
            dst[pl.ds(h, tok, stride=heads), :] = src[:, c] * factor

    for l in range(2):
        meet(l, near[l])
    for l in order[: levels - 2]:
        meet(l, True)
    for l in (1, 0):
        meet(l, jnp.logical_not(near[l]))

    def finish_level(l, ready):
        @pl.when(jnp.logical_and(sends_down(l), ready))
        def _():
            v_copies[l].wait_recv()
            for h, c in enumerate(head):
                g = (wts[l, h] * (dot_nt(vin[l, :, c], og[:, c]) - dots[h])).astype(BF16)
                dsend[l, COMPACT : 2 * COMPACT, c] = (dot_nn(g, q[:, c]) * scale).astype(BF16)
                dq[:, c] += dot_tn(g, kin[l, :, c])
            dk_copies[l].start()

    for l in order:
        offer(l, jnp.logical_not(inside[l]) if l < 2 else True)
    for l in (1, 0):
        finish_level(l, near[l])
    first = [
        jnp.logical_and(
            me // 4 == (1 << l) // 4, spot >= 2 if l == top else True
        )
        for l in range(levels)
    ]
    for l in order[: levels - 2]:
        finish_level(l, first[l])
    for l in landing:

        @pl.when(sends_up(l))
        def _(l=l):
            dv_copies[l].wait_recv()
            dv[...] += dot_nn(pick[l], dvin[l])

    rounded = dv[...].astype(BF16)
    core = lax.rem(me, 2)
    up = lax.rem(me, 4) // 2
    odd = lax.rem(high, 2)
    pair = high // 2
    pairs = quarter // 2
    mate = 2 * pair + 1 - odd
    chunk = 2 * rb
    pieces = send2.shape[1]
    hr = rb // pieces
    others = quarter - 2
    turns, passes = [], []
    for t in range(others):
        there = lax.rem(pair + pairs - t // 2 - 1, pairs)
        above = jnp.where(there > pair, 1, 0)
        turns.append(2 * there + (t % 2) * (1 - above) + (1 - t % 2) * above)
        passes.append(above != odd)
    s1, s2, p_copies, a_copies, b_copies = {}, {}, {}, {}, {}

    def share(t, at, side):
        first = pl.multiple_of((2 * at + side) * chunk, chunk)
        w = dot_nn(xt[pl.ds(first, chunk), :], rounded)
        part[t] = w.reshape(2, rb, cols)
        s1[t] = remote(
            part.at[t, 1 - core], got1.at[t], s1_ss, s1_rs.at[t], flipped(1)
        )
        s1[t].start()

    def halves():
        return [(h, slice(h * hr, (h + 1) * hr)) for h in range(pieces)]

    for t in range(quarter):
        for h in range(pieces):
            s2[t, h] = remote(
                send2.at[t, h], got2.at[t, h], s2_ss.at[t], s2_rs.at[t, h], flipped(2)
            )
    for i in range(2):
        p_copies[i] = remote(psend.at[i], pgot.at[i], p_ss.at[i], p_rs.at[i], tower(mate))

    def cross(t, extra=None):
        s1[t].wait_recv()
        for h, span in halves():
            total = part[t, core, span, :] + got1[t, span, :]
            if extra is not None:
                total = total + extra[span, :].astype(F32)
            send2[t, h] = total.astype(BF16)
            s2[t, h].start()

    def pack(i, t):
        s1[t].wait_recv()
        psend[i] = (part[t, core] + got1[t]).astype(BF16)

    def relay(t):
        at = turns[t]
        s1[quarter + t].wait_recv()
        for h, span in halves():
            s2[t, h].wait_recv()
            kept = part[quarter + t, core, span, :] + got1[quarter + t, span, :]
            kept = kept + got2[t, h].astype(F32)
            a_copies[t, h] = remote(
                zsend.at[t, h], agot.at[t, h], z_ss.at[t], a_rs.at[t, h], tower(mate)
            )
            b_copies[t, h] = remote(
                zsend.at[t, h], bgot.at[t // 2, h], z_ss.at[t], b_rs.at[t // 2, h], tower(at)
            )

            @pl.when(passes[t])
            def _(kept=kept):
                zsend[t, h] = kept.astype(BF16)
                a_copies[t, h].start()

            @pl.when(jnp.logical_not(passes[t]))
            def _(kept=kept):
                a_copies[t, h].wait_recv()
                zsend[t, h] = (kept + agot[t, h].astype(F32)).astype(BF16)
                b_copies[t, h].start()

    far, home = quarter - 1, 2 * quarter - 1
    sender = passes[0]
    joiner = jnp.logical_not(sender)
    eager = jnp.logical_and(joiner, odd == 1)
    hands = jnp.logical_and(eager, up == 0)
    waits = jnp.logical_and(eager, up == 1)
    gives = jnp.logical_not(hands)
    outer = jnp.logical_and(sender, odd == 0)
    takes = jnp.logical_not(jnp.logical_and(outer, up == 0))

    def mate_out():
        s1[home - 1].wait_recv()
        for h, span in halves():
            s2[others, h].wait_recv()
            kept = part[home - 1, core, span, :] + got1[home - 1, span, :]
            psend[1, span, :] = (kept + got2[others, h].astype(F32)).astype(BF16)
        p_copies[1].start()

    share(0, turns[0], 1 - up)
    share(others, mate, 1 - up)
    share(home - 1, mate, up)
    for t in range(1, others):
        share(t, turns[t], 1 - up)
    def give():
        pack(0, others)
        p_copies[0].start()

    pl.when(waits)(give)
    cross(0)
    pl.when(hands)(lambda: cross(others))
    pl.when(jnp.logical_and(gives, jnp.logical_not(waits)))(give)

    @pl.when(jnp.logical_not(waits))
    def _():
        pack(1, home - 1)

    pl.when(hands)(p_copies[1].start)

    for t in range(1, others):
        cross(t)
    for l in landing:
        finish_level(l, jnp.logical_and(joiner, jnp.logical_not((near if l < 2 else first)[l])))
    share(far, high, 1 - up)
    for t in range(others):
        share(quarter + t, turns[t], up)
    share(home, high, up)
    relay(0)
    pl.when(waits)(mate_out)
    pl.when(jnp.logical_not(takes))(lambda: cross(far))

    def cross_home():
        p_copies[0].wait_recv()
        cross(far, pgot.at[0])

    pl.when(jnp.logical_and(takes, jnp.logical_or(joiner, odd == 0)))(cross_home)

    for t in range(1, others):
        relay(t)
    pl.when(jnp.logical_and(sender, odd == 1))(cross_home)
    for l in landing:
        finish_level(l, jnp.logical_and(sender, jnp.logical_not((near if l < 2 else first)[l])))
    pl.when(jnp.logical_not(eager))(p_copies[1].start)
    emit(dq, dq_out, scale)
    emit(dv, dv_out, 1.0)
    dk[...] = dk[...] * scale
    for l in range(levels):

        @pl.when(sends_up(l))
        def _(l=l):
            dk_copies[l].wait_recv()
            dk[...] += dot_nn(pick[l], dkin[l])

    emit(dk, dk_out, 1.0)

    s1[home].wait_recv()
    for h, span in halves():
        s2[far, h].wait_recv()
        total = part[home, core, span, :] + got1[home, span, :]
        wg[span, :] = total + got2[far, h].astype(F32)

    p_copies[1].wait_recv()
    wg[...] += pgot[1].astype(F32)
    def absorb(i):
        for h, span in halves():
            remote(
                zsend.at[i, h], bgot.at[i, h], z_ss.at[i], b_rs.at[i, h], tower(mate)
            ).wait_recv()
            wg[span, :] += bgot[i, h].astype(F32)

    for i in range(pairs - 1):
        absorb(i)

    for l in order:
        fed = remote(kvsend.at[l], kvsend.at[l], up_ss.at[l], k_rs.at[l], to(1 << l))
        pl.when(sends_up(l))(fed.wait_send)
        fed = remote(dsend.at[l], dsend.at[l], down_ss.at[l], dv_rs.at[l], to(-(1 << l)))
        pl.when(sends_down(l))(fed.wait_send)
    remote(part.at[:, 0], got1, s1_ss, s1_rs.at[0], flipped(1)).wait_send()
    for t in range(quarter):
        sent = remote(send2.at[t], got2.at[t], s2_ss.at[t], s2_rs.at[t, 0], flipped(2))
        pl.when(hands if t == others else True)(sent.wait_send)
    for t in range(others):
        sent = remote(zsend.at[t], zsend.at[t], z_ss.at[t], a_rs.at[0, 0], tower(mate))
        sent.wait_send()
    pl.when(gives)(p_copies[0].wait_send)
    p_copies[1].wait_send()


def finish(*refs):
    count = len(refs) // 2
    copies = [
        pltpu.make_async_copy(refs[i], refs[count + i], refs[-1].at[i]) for i in range(count)
    ]
    for copy in copies:
        copy.start()
    for copy in copies:
        copy.wait()


def per_device(queries, keys, values, attended, out_grad, log_sum, picked, layer_input):
    tok, heads, dh = queries.shape
    n = lax.axis_size("kv")
    quarter = n // 4
    levels = n.bit_length() - 1
    cols = heads * dh
    width = layer_input.shape[1]
    rb = width // n
    pieces = min(PIECES, rb // 8)
    rows = (levels + 1 + 7) // 8 * 8
    hbm = pl.BlockSpec(memory_space=pltpu.HBM)
    vmem = pl.BlockSpec(memory_space=pltpu.VMEM)
    sems = pltpu.SemaphoreType.DMA
    level_buf = pltpu.VMEM((levels, COMPACT, cols), BF16)
    out = pl.pallas_call(
        functools.partial(body, n, levels, heads, dh),
        out_shape=[pltpu.VMEM((tok * heads, dh), F32)] * 3 + [pltpu.VMEM((rb, cols), F32)],
        in_specs=[hbm] * 8,
        out_specs=[vmem] * 4,
        scratch_shapes=[
            pltpu.SMEM(picked.shape, jnp.int32),
            pltpu.VMEM((heads, tok), F32),
            pltpu.VMEM((tok, cols), F32),
            pltpu.VMEM((tok, cols), F32),
            pltpu.VMEM((tok, cols), F32),
            pltpu.VMEM((5, tok, heads, dh), BF16),
        ]
        + [pltpu.VMEM((tok, cols), BF16)] * 5
        + [
            pltpu.VMEM((tok, width), BF16),
            pltpu.VMEM((width, tok), BF16),
            pltpu.VMEM((rows, tok), F32),
            pltpu.VMEM((levels, rows, tok), F32),
            pltpu.VMEM((levels, tok, COMPACT), BF16),
        ]
        + [pltpu.VMEM((levels, 2, COMPACT, cols), BF16), level_buf, level_buf]
        + [pltpu.VMEM((levels, 2 * COMPACT + 2 * rows * tok // cols, cols), BF16)]
        + [level_buf] * 2
        + [
            pltpu.VMEM((levels, heads, COMPACT, tok), F32),
            pltpu.VMEM((n // 2, 2, rb, cols), F32),
            pltpu.VMEM((n // 2, rb, cols), F32),
            pltpu.VMEM((quarter, pieces, rb // pieces, cols), BF16),
            pltpu.VMEM((quarter, pieces, rb // pieces, cols), BF16),
            pltpu.VMEM((2, rb, cols), BF16),
            pltpu.VMEM((2, rb, cols), BF16),
            pltpu.VMEM((quarter - 2, pieces, rb // pieces, cols), BF16),
            pltpu.VMEM((quarter - 2, pieces, rb // pieces, cols), BF16),
            pltpu.VMEM((quarter // 2 - 1, pieces, rb // pieces, cols), BF16),
            sems,
            sems,
            sems,
            sems((5,)),
        ]
        + [sems((levels,))] * 7
        + [
            sems,
            sems((n // 2,)),
            sems((quarter,)),
            sems((quarter, pieces)),
            sems((2,)),
            sems((2,)),
            sems((quarter - 2,)),
            sems((quarter - 2, pieces)),
            sems((quarter // 2 - 1, pieces)),
        ],
        compiler_params=pltpu.CompilerParams(
            collective_id=0, has_side_effects=True
        ),
    )(picked, queries, keys, values, attended, out_grad, log_sum.T, layer_input)
    dq, dk, dv, wg = pl.pallas_call(
        finish,
        out_shape=[jax.ShapeDtypeStruct(o.shape, F32) for o in out],
        in_specs=[vmem] * 4,
        out_specs=[hbm] * 4,
        scratch_shapes=[sems((4,))],
    )(*(pltpu.with_memory_space_constraint(o, pltpu.VMEM) for o in out))
    return *(g.reshape(tok, heads, dh) for g in (dq, dk, dv)), wg


def solution(mesh):
    placed = (P("kv", "tp", None),) * 5 + (P("kv", "tp"), P("kv", None), P("kv", None))
    return jax.shard_map(
        per_device,
        mesh=mesh,
        in_specs=placed,
        out_specs=(P("kv", "tp", None), P("kv", "tp", None), P("kv", "tp", None), P("kv", "tp")),
        check_vma=False,
    )
```

```python
import functools

import jax
import jax.numpy as jnp
from jax import lax
from jax.experimental import pallas as pl
from jax.experimental.pallas import tpu as pltpu
from jax.sharding import PartitionSpec as P

QB = 128
KB = 32
PER_SPAN = 4
COMPACT = PER_SPAN * KB
CHUNKS = 8
PIECES = 4
F32 = jnp.float32
BF16 = jnp.bfloat16


def xor(value, bits):
    out = value
    for i in range(bits.bit_length()):
        if bits >> i & 1:
            out = out + (1 << i) - (2 << i) * lax.rem(value // (1 << i), 2)
    return out


def dot_nt(a, b):
    return lax.dot_general(a, b, (((1,), (1,)), ((), ())), preferred_element_type=F32)


def dot_tn(a, b):
    return lax.dot_general(a, b, (((0,), (0,)), ((), ())), preferred_element_type=F32)


def dot_nn(a, b):
    return lax.dot_general(a, b, (((1,), (0,)), ((), ())), preferred_element_type=F32)


def body(
    n, levels, heads, dh,
    picked_hbm, q_hbm, k_hbm, v_hbm, att_hbm, og_hbm, log_hbm, x_hbm,
    dq_out, dk_out, dv_out, wg,
    picked, log_sum, dq, dk, dv, raw, q, k, v, att, og, x, xt, slot, slot_in, pick, kvsend, kin, vin, dsend, dvin, dkin,
    wts, part, got1, send2, got2, psend, pgot, zsend, agot, bgot,
    x_sem, picked_sem, log_sem, raw_sem, up_ss, down_ss, slot_rs, k_rs, v_rs, dv_rs, dk_rs,
    s1_ss, s1_rs, s2_ss, s2_rs, p_ss, p_rs, z_ss, a_rs, b_rs,
):
    me = lax.axis_index("kv")
    tok, cols = q.shape
    query_count = tok // QB
    span_blocks = tok // KB
    rows = slot.shape[0]
    scale = dh ** (-0.5)
    quarter = n // 4
    rb = wg.shape[0]
    top = levels - 1
    order = list(reversed(range(levels)))
    landing = order

    def to(offset):
        return {"kv": lax.rem(me + offset + n, n)}

    def flipped(bits):
        low = lax.rem(me, 4)
        if bits == 1:
            return {"kv": me + 1 - 2 * lax.rem(me, 2)}
        return {"kv": me + 2 - 4 * (low // 2)}

    def tower(at):
        return {"kv": at * 4 + lax.rem(me, 4)}

    def remote(src, dst, ss, rs, device):
        return pltpu.make_async_remote_copy(
            src_ref=src, dst_ref=dst, send_sem=ss, recv_sem=rs,
            device_id=device, device_id_type=pl.DeviceIdType.MESH,
        )

    load_picked = pltpu.make_async_copy(picked_hbm, picked, picked_sem)
    load_picked.start()
    barrier = pltpu.get_barrier_semaphore()
    greeted = [to(1 << l) for l in range(levels)] + [to(-(1 << l)) for l in range(levels)]
    high = me // 4
    greeted += [flipped(1), flipped(2)]
    greeted += [tower(lax.rem(high + b, quarter)) for b in range(1, quarter)]
    for device in greeted:
        pl.semaphore_signal(
            barrier, inc=1, device_id=device, device_id_type=pl.DeviceIdType.MESH
        )

    loads = {}
    for i, (src, dst) in enumerate(
        ((k_hbm, k), (v_hbm, v), (q_hbm, q), (og_hbm, og), (att_hbm, att))
    ):
        loads[i] = (pltpu.make_async_copy(src, raw.at[i], raw_sem.at[i]), dst)
        loads[i][0].start()

    def settle(i):
        copy, dst = loads[i]
        copy.wait()
        for h in range(heads):
            dst[:, h * dh : (h + 1) * dh] = raw[i, :, h, :]

    load_x = pltpu.make_async_copy(x_hbm, x, x_sem)
    load_x.start()
    load_log = pltpu.make_async_copy(log_hbm, log_sum, log_sem)
    load_log.start()
    row = lax.broadcasted_iota(jnp.int32, (rows, tok), 0)
    lane = lax.broadcasted_iota(jnp.int32, (rows, tok), 1)
    back = jnp.zeros((rows, tok), jnp.int32)
    for l in range(levels):
        back = jnp.where(row == l + 1, 1 << l, back)
    ids = jnp.where(row <= levels, (me - back) * span_blocks + lane // KB, -2)
    load_picked.wait()
    live = []
    for b in range(query_count):
        hit = jnp.zeros((rows, tok), jnp.int32)
        for s in range(picked.shape[1]):
            p = picked[b, s]
            hit = jnp.where(ids == jnp.where(p < 0, -(1 << 30), p), 1, hit)
        live.append(hit.astype(F32))
    need = functools.reduce(jnp.maximum, live)
    below = lax.broadcasted_iota(jnp.int32, (tok, tok), 0)
    above = lax.broadcasted_iota(jnp.int32, (tok, tok), 1)
    steps = jnp.where((below % KB == 0) & (below // KB < above // KB), 1.0, 0.0).astype(BF16)
    rank = dot_nn(need.astype(BF16), steps)
    slot[...] = jnp.where(need > 0, rank * KB + (lane % KB).astype(F32), -1.0)

    pl.semaphore_wait(barrier, len(greeted))

    def sends_up(l):
        return me + (1 << l) < n

    def sends_down(l):
        return me >= 1 << l

    slot_copies = {}
    for l in order:
        slot_copies[l] = remote(
            slot, slot_in.at[l], down_ss.at[l], slot_rs.at[l], to(-(1 << l))
        )
        pl.when(sends_down(l))(slot_copies[l].start)

    k_copies, v_copies, dv_copies, dk_copies = {}, {}, {}, {}
    for l in order:
        k_copies[l] = remote(
            kvsend.at[l, 0], kin.at[l], up_ss.at[l], k_rs.at[l], to(1 << l)
        )
    settle(0)
    settle(1)

    def one_hot(row_values):
        sub = lax.broadcasted_iota(jnp.int32, (COMPACT, tok), 0).astype(F32)
        return jnp.where(sub == row_values, 1.0, 0.0).astype(BF16)

    head = [slice(h * dh, (h + 1) * dh) for h in range(heads)]
    for l in order:
        v_copies[l] = remote(
            kvsend.at[l, 1], vin.at[l], up_ss.at[l], v_rs.at[l], to(1 << l)
        )
        dv_copies[l] = remote(
            dsend.at[l, :COMPACT], dvin.at[l], down_ss.at[l], dv_rs.at[l], to(-(1 << l))
        )
        dk_copies[l] = remote(
            dsend.at[l, COMPACT : 2 * COMPACT], dkin.at[l], down_ss.at[l], dk_rs.at[l],
            to(-(1 << l)),
        )
    for l in order[: levels - 2] + [0, 1]:

        @pl.when(sends_up(l))
        def _(l=l):
            slot_copies[l].wait_recv()
            chosen = one_hot(slot_in[l, l + 1 : l + 2, :])
            kvsend[l, 0] = dot_nn(chosen, k[...]).astype(BF16)
            k_copies[l].start()
            pick[l] = jnp.transpose(chosen)
            kvsend[l, 1] = dot_nn(chosen, v[...]).astype(BF16)

    spot = lax.rem(me, 4)
    near = [spot >= 1 << l for l in range(2)]
    inside = [spot + (1 << l) < 4 for l in range(2)]

    def offer(l, ready):
        @pl.when(jnp.logical_and(sends_up(l), ready))
        def _():
            v_copies[l].start()

    for l in range(2):
        offer(l, inside[l])
    for i in range(2, 5):
        settle(i)
    dots = []
    for c in head:
        column = jnp.sum(og[:, c].astype(F32) * att[:, c].astype(F32), axis=1, keepdims=True)
        dots.append(jnp.transpose(jnp.broadcast_to(column, (tok, 128)))[0:1, :])
    load_log.wait()
    stored = [log_sum[h : h + 1, :] for h in range(heads)]

    def key_mask(chosen, r):
        pieces = []
        for m in live:
            column = dot_nt(chosen, m.astype(BF16))[:, r : r + 1]
            pieces.append(jnp.broadcast_to(column, (column.shape[0], QB)))
        return jnp.concatenate(pieces, axis=1) > 0

    own_mask = key_mask(jnp.where(below == above, 1.0, 0.0).astype(BF16), 0) & (below <= above)
    for h, c in enumerate(head):
        w = jnp.where(own_mask, jnp.exp(dot_nt(k[:, c], q[:, c]) * scale - stored[h]), 0.0)
        dv[:, c] = dot_nn(w.astype(BF16), og[:, c])
        g = (w * (dot_nt(v[:, c], og[:, c]) - dots[h])).astype(BF16)
        dk[:, c] = dot_nn(g, q[:, c])
        dq[:, c] = dot_tn(g, k[:, c])

    masks = {l: key_mask(one_hot(slot[l + 1 : l + 2, :]), l + 1) for l in order}
    load_x.wait()
    width = x.shape[1] // CHUNKS
    for i in range(CHUNKS):
        xt[i * width : (i + 1) * width, :] = jnp.transpose(x[:, i * width : (i + 1) * width])
    def meet(l, ready):
        @pl.when(jnp.logical_and(sends_down(l), ready))
        def _():
            k_copies[l].wait_recv()
            for h, c in enumerate(head):
                w = jnp.where(
                    masks[l], jnp.exp(dot_nt(kin[l, :, c], q[:, c]) * scale - stored[h]), 0.0
                )
                wts[l, h] = w
                dsend[l, :COMPACT, c] = dot_nn(w.astype(BF16), og[:, c]).astype(BF16)
            dv_copies[l].start()

    def emit(src, dst, factor):
        for h, c in enumerate(head):
            dst[pl.ds(h, tok, stride=heads), :] = src[:, c] * factor

    for l in range(2):
        meet(l, near[l])
    for l in order[: levels - 2]:
        meet(l, True)
    for l in (1, 0):
        meet(l, jnp.logical_not(near[l]))

    def finish_level(l, ready):
        @pl.when(jnp.logical_and(sends_down(l), ready))
        def _():
            v_copies[l].wait_recv()
            for h, c in enumerate(head):
                g = (wts[l, h] * (dot_nt(vin[l, :, c], og[:, c]) - dots[h])).astype(BF16)
                dsend[l, COMPACT : 2 * COMPACT, c] = (dot_nn(g, q[:, c]) * scale).astype(BF16)
                dq[:, c] += dot_tn(g, kin[l, :, c])
            dk_copies[l].start()

    for l in order:
        offer(l, jnp.logical_not(inside[l]) if l < 2 else True)
    for l in (1, 0):
        finish_level(l, near[l])
    first = [
        jnp.logical_and(
            me // 4 == (1 << l) // 4, spot >= 2 if l == top else True
        )
        for l in range(levels)
    ]
    for l in order[: levels - 2]:
        finish_level(l, first[l])
    for l in landing:

        @pl.when(sends_up(l))
        def _(l=l):
            dv_copies[l].wait_recv()
            dv[...] += dot_nn(pick[l], dvin[l])

    rounded = dv[...].astype(BF16)
    core = lax.rem(me, 2)
    up = lax.rem(me, 4) // 2
    odd = lax.rem(high, 2)
    pair = high // 2
    pairs = quarter // 2
    mate = 2 * pair + 1 - odd
    chunk = 2 * rb
    pieces = send2.shape[1]
    hr = rb // pieces
    others = quarter - 2
    turns, passes = [], []
    for t in range(others):
        there = lax.rem(pair + pairs - t // 2 - 1, pairs)
        above = jnp.where(there > pair, 1, 0)
        turns.append(2 * there + (t % 2) * (1 - above) + (1 - t % 2) * above)
        passes.append(above != odd)
    s1, s2, p_copies, a_copies, b_copies = {}, {}, {}, {}, {}

    def share(t, at, side):
        first = pl.multiple_of((2 * at + side) * chunk, chunk)
        w = dot_nn(xt[pl.ds(first, chunk), :], rounded)
        part[t] = w.reshape(2, rb, cols)
        s1[t] = remote(
            part.at[t, 1 - core], got1.at[t], s1_ss, s1_rs.at[t], flipped(1)
        )
        s1[t].start()

    def halves():
        return [(h, slice(h * hr, (h + 1) * hr)) for h in range(pieces)]

    for t in range(quarter):
        for h in range(pieces):
            s2[t, h] = remote(
                send2.at[t, h], got2.at[t, h], s2_ss.at[t], s2_rs.at[t, h], flipped(2)
            )
    for i in range(2):
        p_copies[i] = remote(psend.at[i], pgot.at[i], p_ss.at[i], p_rs.at[i], tower(mate))

    def cross(t, extra=None):
        s1[t].wait_recv()
        for h, span in halves():
            total = part[t, core, span, :] + got1[t, span, :]
            if extra is not None:
                total = total + extra[span, :].astype(F32)
            send2[t, h] = total.astype(BF16)
            s2[t, h].start()

    def pack(i, t):
        s1[t].wait_recv()
        psend[i] = (part[t, core] + got1[t]).astype(BF16)

    def relay(t):
        at = turns[t]
        s1[quarter + t].wait_recv()
        for h, span in halves():
            s2[t, h].wait_recv()
            kept = part[quarter + t, core, span, :] + got1[quarter + t, span, :]
            kept = kept + got2[t, h].astype(F32)
            a_copies[t, h] = remote(
                zsend.at[t, h], agot.at[t, h], z_ss, a_rs.at[t, h], tower(mate)
            )
            b_copies[t, h] = remote(
                zsend.at[t, h], bgot.at[t // 2, h], z_ss, b_rs.at[t // 2, h], tower(at)
            )

            @pl.when(passes[t])
            def _(kept=kept):
                zsend[t, h] = kept.astype(BF16)
                a_copies[t, h].start()

            @pl.when(jnp.logical_not(passes[t]))
            def _(kept=kept):
                a_copies[t, h].wait_recv()
                zsend[t, h] = (kept + agot[t, h].astype(F32)).astype(BF16)
                b_copies[t, h].start()

    far, home = quarter - 1, 2 * quarter - 1
    sender = passes[0]
    joiner = jnp.logical_not(sender)
    eager = jnp.logical_and(joiner, odd == 1)
    hands = jnp.logical_and(eager, up == 0)
    waits = jnp.logical_and(eager, up == 1)
    gives = jnp.logical_not(hands)
    outer = jnp.logical_and(sender, odd == 0)
    takes = jnp.logical_not(jnp.logical_and(outer, up == 0))

    def mate_out():
        s1[home - 1].wait_recv()
        for h, span in halves():
            s2[others, h].wait_recv()
            kept = part[home - 1, core, span, :] + got1[home - 1, span, :]
            psend[1, span, :] = (kept + got2[others, h].astype(F32)).astype(BF16)
        p_copies[1].start()

    share(0, turns[0], 1 - up)
    share(others, mate, 1 - up)
    share(home - 1, mate, up)
    for t in range(1, others):
        share(t, turns[t], 1 - up)
    def give():
        pack(0, others)
        p_copies[0].start()

    pl.when(waits)(give)
    cross(0)
    pl.when(hands)(lambda: cross(others))
    pl.when(jnp.logical_and(gives, jnp.logical_not(waits)))(give)

    @pl.when(jnp.logical_not(waits))
    def _():
        pack(1, home - 1)

    pl.when(hands)(p_copies[1].start)

    for t in range(1, others):
        cross(t)
    for l in landing:
        finish_level(l, jnp.logical_and(joiner, jnp.logical_not((near if l < 2 else first)[l])))
    share(far, high, 1 - up)
    for t in range(others):
        share(quarter + t, turns[t], up)
    share(home, high, up)
    relay(0)
    pl.when(waits)(mate_out)
    pl.when(jnp.logical_not(takes))(lambda: cross(far))

    def cross_home():
        p_copies[0].wait_recv()
        cross(far, pgot.at[0])

    pl.when(jnp.logical_and(takes, jnp.logical_or(joiner, odd == 0)))(cross_home)

    for t in range(1, others):
        relay(t)
    pl.when(jnp.logical_and(sender, odd == 1))(cross_home)
    for l in landing:
        finish_level(l, jnp.logical_and(sender, jnp.logical_not((near if l < 2 else first)[l])))
    pl.when(jnp.logical_not(eager))(p_copies[1].start)
    emit(dq, dq_out, scale)
    emit(dv, dv_out, 1.0)
    dk[...] = dk[...] * scale
    for l in range(levels):

        @pl.when(sends_up(l))
        def _(l=l):
            dk_copies[l].wait_recv()
            dk[...] += dot_nn(pick[l], dkin[l])

    emit(dk, dk_out, 1.0)

    s1[home].wait_recv()
    for h, span in halves():
        s2[far, h].wait_recv()
        total = part[home, core, span, :] + got1[home, span, :]
        wg[span, :] = total + got2[far, h].astype(F32)

    p_copies[1].wait_recv()
    wg[...] += pgot[1].astype(F32)
    def absorb(i):
        for h, span in halves():
            remote(
                zsend.at[i, h], bgot.at[i, h], z_ss, b_rs.at[i, h], tower(mate)
            ).wait_recv()
            wg[span, :] += bgot[i, h].astype(F32)

    for i in range(pairs - 1):
        absorb(i)

    for l in order:
        fed = remote(kvsend.at[l], kvsend.at[l], up_ss.at[l], k_rs.at[l], to(1 << l))
        pl.when(sends_up(l))(fed.wait_send)
        fed = remote(dsend.at[l], dsend.at[l], down_ss.at[l], dv_rs.at[l], to(-(1 << l)))
        pl.when(sends_down(l))(fed.wait_send)
    remote(part.at[:, 0], got1, s1_ss, s1_rs.at[0], flipped(1)).wait_send()
    for t in range(quarter):
        sent = remote(send2.at[t], got2.at[t], s2_ss.at[t], s2_rs.at[t, 0], flipped(2))
        pl.when(hands if t == others else True)(sent.wait_send)
    remote(zsend, zsend, z_ss, a_rs.at[0, 0], tower(mate)).wait_send()
    pl.when(gives)(p_copies[0].wait_send)
    p_copies[1].wait_send()


def finish(*refs):
    count = len(refs) // 2
    copies = [
        pltpu.make_async_copy(refs[i], refs[count + i], refs[-1].at[i]) for i in range(count)
    ]
    for copy in copies:
        copy.start()
    for copy in copies:
        copy.wait()


def per_device(queries, keys, values, attended, out_grad, log_sum, picked, layer_input):
    tok, heads, dh = queries.shape
    n = lax.axis_size("kv")
    quarter = n // 4
    levels = n.bit_length() - 1
    cols = heads * dh
    width = layer_input.shape[1]
    rb = width // n
    pieces = min(PIECES, rb // 8)
    rows = (levels + 1 + 7) // 8 * 8
    hbm = pl.BlockSpec(memory_space=pltpu.HBM)
    vmem = pl.BlockSpec(memory_space=pltpu.VMEM)
    sems = pltpu.SemaphoreType.DMA
    level_buf = pltpu.VMEM((levels, COMPACT, cols), BF16)
    out = pl.pallas_call(
        functools.partial(body, n, levels, heads, dh),
        out_shape=[pltpu.VMEM((tok * heads, dh), F32)] * 3 + [pltpu.VMEM((rb, cols), F32)],
        in_specs=[hbm] * 8,
        out_specs=[vmem] * 4,
        scratch_shapes=[
            pltpu.SMEM(picked.shape, jnp.int32),
            pltpu.VMEM((heads, tok), F32),
            pltpu.VMEM((tok, cols), F32),
            pltpu.VMEM((tok, cols), F32),
            pltpu.VMEM((tok, cols), F32),
            pltpu.VMEM((5, tok, heads, dh), BF16),
        ]
        + [pltpu.VMEM((tok, cols), BF16)] * 5
        + [
            pltpu.VMEM((tok, width), BF16),
            pltpu.VMEM((width, tok), BF16),
            pltpu.VMEM((rows, tok), F32),
            pltpu.VMEM((levels, rows, tok), F32),
            pltpu.VMEM((levels, tok, COMPACT), BF16),
        ]
        + [pltpu.VMEM((levels, 2, COMPACT, cols), BF16), level_buf, level_buf]
        + [pltpu.VMEM((levels, 2 * COMPACT + 2 * rows * tok // cols, cols), BF16)]
        + [level_buf] * 2
        + [
            pltpu.VMEM((levels, heads, COMPACT, tok), F32),
            pltpu.VMEM((n // 2, 2, rb, cols), F32),
            pltpu.VMEM((n // 2, rb, cols), F32),
            pltpu.VMEM((quarter, pieces, rb // pieces, cols), BF16),
            pltpu.VMEM((quarter, pieces, rb // pieces, cols), BF16),
            pltpu.VMEM((2, rb, cols), BF16),
            pltpu.VMEM((2, rb, cols), BF16),
            pltpu.VMEM((quarter - 2, pieces, rb // pieces, cols), BF16),
            pltpu.VMEM((quarter - 2, pieces, rb // pieces, cols), BF16),
            pltpu.VMEM((quarter // 2 - 1, pieces, rb // pieces, cols), BF16),
            sems,
            sems,
            sems,
            sems((5,)),
        ]
        + [sems((levels,))] * 7
        + [
            sems,
            sems((n // 2,)),
            sems((quarter,)),
            sems((quarter, pieces)),
            sems((2,)),
            sems((2,)),
            sems,
            sems((quarter - 2, pieces)),
            sems((quarter // 2 - 1, pieces)),
        ],
        compiler_params=pltpu.CompilerParams(
            collective_id=0, has_side_effects=True
        ),
    )(picked, queries, keys, values, attended, out_grad, log_sum.T, layer_input)
    dq, dk, dv, wg = pl.pallas_call(
        finish,
        out_shape=[jax.ShapeDtypeStruct(o.shape, F32) for o in out],
        in_specs=[vmem] * 4,
        out_specs=[hbm] * 4,
        scratch_shapes=[sems((4,))],
    )(*(pltpu.with_memory_space_constraint(o, pltpu.VMEM) for o in out))
    return *(g.reshape(tok, heads, dh) for g in (dq, dk, dv)), wg


def solution(mesh):
    placed = (P("kv", "tp", None),) * 5 + (P("kv", "tp"), P("kv", None), P("kv", None))
    return jax.shard_map(
        per_device,
        mesh=mesh,
        in_specs=placed,
        out_specs=(P("kv", "tp", None), P("kv", "tp", None), P("kv", "tp", None), P("kv", "tp")),
        check_vma=False,
    )
```
